32 devices in a mesh: st: 16 (over z, y, x), tp: 2 (over core).
Axes of the slice: x: 2, y: 2, z: 4, core: 2. Of those that a mesh axis runs over, the one named last changes fastest.
Arguments:
- tokens: bfloat16 [4096, 2048], P('st'), may hold values from -6 to 6
- store: bfloat16 [64, 64, 2048], P('st'), may hold values from -6 to 6
- passage_ids: int32 [64, 4], P('st'), may hold values from 0 to 63, as said below
- w_query: bfloat16 [2048, 2048], P(None, 'tp'), may hold values from -0.125 to 0.125
- w_key: bfloat16 [2048, 512], P(None, 'tp'), may hold values from -0.125 to 0.125
- w_value: bfloat16 [2048, 512], P(None, 'tp'), may hold values from -0.125 to 0.125
- w_ret_query: bfloat16 [2048, 1024], P(None, 'tp'), may hold values from -0.125 to 0.125
- w_ret_key: bfloat16 [2048, 1024], P(None, 'tp'), may hold values from -0.125 to 0.125
- w_ret_value: bfloat16 [2048, 2048], P(None, 'tp'), may hold values from -0.125 to 0.125
- ret_rate: float32 [8], P('tp'), may hold values from 0.003 to 0.03
- ret_gain: float32 [2048], P('tp'), may hold values from 0.1 to 1.9
- gate_logit: float32 [2048], P('tp'), may hold values from -2 to 2
- out_grad: bfloat16 [4096, 2048], P('st', 'tp'), may hold values from -6 to 6
Outputs:
- grad_tokens: bfloat16 [4096, 2048], P(('st', 'tp'))
- grad_store: bfloat16 [64, 64, 2048], P(('st', 'tp'))
- grad_key_weight: float32 [2048, 512], P(None, 'tp')
The draws below stay inside these ranges and needn't reach their ends.
Inputs may be any that keep to these rules, and one draw needn't show every extreme that they name: `passage_ids`: passage p lies on index p // 4 of st. The rows of one device name exactly 1 passage of every owner, so the 4 passages of a block differ.
All inputs are finite; a program needn't handle non-finite values.
Results may differ from the reference program's by a relative error of at most 0.012.
Values may be sent and summed in bfloat16 or wider, within the bound.
A program may use at most 192 MiB of HBM per device.

```python
import math
import jax
import jax.numpy as jnp
from jax import lax

D = 2048
HEADS = 8
HEAD = 256
KV_HEADS = 2
RET_HEADS = 8
RET_KEY = 128
RET_VALUE = 256
BLK = 64
KP = 4
PLEN = 64
PASS_DEV = 4
TOK_DEV = 256
TOKENS = 4096
BLOCKS = 64
PASSAGES = 64
N_ST = 16


def draw_passage_ids(key, part):

    def for_reader(reader):
        stream = jax.random.fold_in(jax.random.fold_in(key, 7), reader)
        first, second, third = jax.random.split(stream, 3)
        owner = jax.random.permutation(first, N_ST).astype(jnp.int32)
        local = jnp.minimum(jax.random.randint(second, (N_ST,), 0, PASS_DEV), jax.random.randint(third, (N_ST,), 0, PASS_DEV))
        return (owner * PASS_DEV + local).astype(jnp.int32)
    every = jax.vmap(for_reader)(jnp.arange(N_ST, dtype=jnp.int32))
    return every.reshape(BLOCKS, KP)


def shard_levels(own_key, dims, pieces, least, top_value):
    gain = 1.0
    for axis_at, blocks in pieces:
        steps = jax.random.uniform(jax.random.fold_in(jax.random.fold_in(own_key, 6), axis_at), (blocks,), jnp.float32, least / len(pieces), top_value / len(pieces))
        gain = gain * jnp.repeat(jnp.exp(steps), dims[axis_at] // blocks).reshape((-1,) + (1,) * (len(dims) - 1 - axis_at))
    return gain


def scatter_about(rng, extent, spread, bound, pieces=(), kind=jnp.bfloat16):
    values = jax.random.normal(rng, extent, jnp.float32) * spread
    if len(pieces) > 0:
        values = shard_levels(rng, extent, pieces, -0.22, 0.18) * values
    return jnp.clip(values, min=-bound, max=bound).astype(kind)


def setup_inputs(seed: int = 0) -> dict:
    key_list = jax.random.split(jax.random.key(seed), 14)
    tokens = scatter_about(key_list[0], (TOKENS, D), 1.0, 6.0, ((0, 16),))
    store = scatter_about(key_list[1], (PASSAGES, PLEN, D), 1.0, 6.0, ((0, 16),))
    passage_ids = draw_passage_ids(jax.random.fold_in(key_list[13], 71), 0)
    w_query = scatter_about(key_list[3], (D, HEADS * HEAD), D ** -0.5, 0.125, ((1, 2),))
    w_key = scatter_about(key_list[4], (D, KV_HEADS * HEAD), D ** -0.5, 0.125, ((1, 2),))
    w_value = scatter_about(key_list[5], (D, KV_HEADS * HEAD), D ** -0.5, 0.125, ((1, 2),))
    w_ret_query = scatter_about(key_list[6], (D, RET_HEADS * RET_KEY), D ** -0.5, 0.125, ((1, 2),))
    w_ret_key = scatter_about(key_list[7], (D, RET_HEADS * RET_KEY), D ** -0.5, 0.125, ((1, 2),))
    w_ret_value = scatter_about(key_list[8], (D, RET_HEADS * RET_VALUE), D ** -0.5, 0.125, ((1, 2),))
    ret_rate = jnp.clip(jnp.exp(math.log(0.03) - 2.3025851 * jax.random.uniform(key_list[9], (RET_HEADS,), jnp.float32) ** shard_levels(key_list[9], (RET_HEADS,), ((0, 2),), -0.2, 0.2)), 0.003, 0.03)
    ret_gain = jnp.clip(1.0 + 0.18 * jax.random.normal(key_list[10], (D,), jnp.float32), 0.1, 1.9)
    gate_logit = jnp.clip(jax.random.uniform(key_list[11], (D,), jnp.float32, -2.0, 2.0) * shard_levels(key_list[11], (D,), ((0, 2),), -0.4, 0.0), -2.0, 2.0)
    out_grad = scatter_about(key_list[12], (TOKENS, D), 1.0, 6.0, ((0, 16), (1, 2)))
    return {"tokens": tokens, "store": store, "passage_ids": passage_ids, "w_query": w_query, "w_key": w_key, "w_value": w_value, "w_ret_query": w_ret_query, "w_ret_key": w_ret_key, "w_ret_value": w_ret_value, "ret_rate": ret_rate, "ret_gain": ret_gain, "gate_logit": gate_logit, "out_grad": out_grad}


EPSILON = 1.0
HIGH = lax.Precision.HIGHEST

def rounded(values):
    return lax.optimization_barrier(values.astype(jnp.bfloat16)).astype(jnp.float32)

def retention_grads(query_rows, key_rows, value_rows, rates, gains, cotangent):
    length = query_rows.shape[0]
    heads = rates.shape[0]
    queries = query_rows.astype(jnp.float32).reshape(length, heads, -1)
    keyset = key_rows.astype(jnp.float32).reshape(length, heads, -1)
    values = value_rows.astype(jnp.float32).reshape(length, heads, -1)
    positions = jnp.arange(length, dtype=jnp.float32)
    distance = positions[:, None] - positions[None, :]
    damping = jnp.where(distance >= 0.0, jnp.exp(-rates[:, None, None] * jnp.maximum(distance, 0.0)), 0.0) * queries.shape[-1] ** (-0.5)
    raw = jnp.einsum('thd,shd->hts', queries, keyset, precision=HIGH)
    weights = rounded(raw * damping)
    mixed = jnp.einsum('hts,she->the', weights, values, precision=HIGH)
    inverse = lax.rsqrt(lax.optimization_barrier(jnp.mean(mixed * mixed, axis=-1, keepdims=True)) + EPSILON)
    scaled = cotangent.astype(jnp.float32).reshape(length, heads, -1) * gains.reshape(heads, -1)
    inner = lax.optimization_barrier(jnp.mean(scaled * mixed, axis=-1, keepdims=True))
    grad_mixed = rounded(inverse * scaled - inverse * inverse * inverse * mixed * inner)
    grad_weights = rounded(jnp.einsum('the,she->hts', grad_mixed, values, precision=HIGH) * damping)
    grad_first = jnp.einsum('hts,shd->thd', grad_weights, keyset, precision=HIGH).astype(jnp.bfloat16).reshape(length, -1)
    grad_second = jnp.einsum('hts,thd->shd', grad_weights, queries, precision=HIGH).astype(jnp.bfloat16).reshape(length, -1)
    grad_third = jnp.einsum('hts,the->she', weights, grad_mixed, precision=HIGH).astype(jnp.bfloat16).reshape(length, -1)
    return (grad_first, grad_second, grad_third)

def reference(tokens, store, passage_ids, w_query, w_key, w_value, w_ret_query, w_ret_key, w_ret_value, ret_rate, ret_gain, gate_logit, out_grad):
    count, plen, width = store.shape
    kv_width = w_key.shape[1]
    kv_heads = kv_width // HEAD
    group = w_query.shape[1] // HEAD // kv_heads
    flat_store = store.reshape(count * plen, width)
    key_table = jnp.dot(flat_store, w_key, preferred_element_type=jnp.float32).astype(jnp.bfloat16).reshape(count, plen, kv_width)
    value_table = jnp.dot(flat_store, w_value, preferred_element_type=jnp.float32).astype(jnp.bfloat16).reshape(count, plen, kv_width)
    gate = jax.nn.sigmoid(gate_logit)
    blocks_dev = TOK_DEV // BLK
    seq_tokens = tokens.reshape(N_ST, TOK_DEV, width)
    seq_ids = passage_ids.reshape(N_ST, blocks_dev * KP)
    seq_grad = out_grad.reshape(N_ST, TOK_DEV, width)
    factor = HEAD ** (-0.5)

    def per_sequence(carry, inputs):
        rows, ids, grad_rows = inputs
        query_bf = jnp.dot(rows, w_query, preferred_element_type=jnp.float32).astype(jnp.bfloat16)
        keys = key_table[ids].reshape(blocks_dev, KP * plen, kv_heads, HEAD).astype(jnp.float32)
        values = value_table[ids].reshape(blocks_dev, KP * plen, kv_heads, HEAD).astype(jnp.float32)
        queries = query_bf.reshape(blocks_dev, BLK, kv_heads, group, HEAD).astype(jnp.float32)
        scores = jnp.einsum('btkgd,bskd->bkgts', queries, keys, precision=HIGH) * factor
        expo = jnp.exp(scores)
        probs = expo / lax.optimization_barrier(jnp.sum(expo, axis=-1, keepdims=True))
        probs_bf = rounded(probs)
        attn = jnp.einsum('bkgts,bskd->btkgd', probs_bf, values, precision=HIGH)
        grad_attn = grad_rows.astype(jnp.float32).reshape(blocks_dev, BLK, kv_heads, group, HEAD) * gate.reshape(kv_heads, group, HEAD)
        grad_attn_bf = rounded(grad_attn)
        grad_probs = jnp.einsum('btkgd,bskd->bkgts', grad_attn_bf, values, precision=HIGH)
        delta = jnp.einsum('btkgd,btkgd->bkgt', grad_attn, attn, precision=HIGH)
        grad_scores = rounded(probs * (grad_probs - delta[..., None]) * factor)
        grad_query = jnp.einsum('bkgts,bskd->btkgd', grad_scores, keys, precision=HIGH).astype(jnp.bfloat16).reshape(TOK_DEV, -1)
        grad_keys = jnp.einsum('bkgts,btkgd->bskd', grad_scores, queries, precision=HIGH).astype(jnp.bfloat16).reshape(blocks_dev * KP, plen, kv_width)
        grad_values = jnp.einsum('bkgts,btkgd->bskd', probs_bf, grad_attn_bf, precision=HIGH).astype(jnp.bfloat16).reshape(blocks_dev * KP, plen, kv_width)
        ret_query = jnp.dot(rows, w_ret_query, preferred_element_type=jnp.float32).astype(jnp.bfloat16)
        ret_key = jnp.dot(rows, w_ret_key, preferred_element_type=jnp.float32).astype(jnp.bfloat16)
        ret_value = jnp.dot(rows, w_ret_value, preferred_element_type=jnp.float32).astype(jnp.bfloat16)
        grad_rq, grad_rk, grad_rv = retention_grads(ret_query, ret_key, ret_value, ret_rate, ret_gain, grad_rows)
        grad_rows_out = (jnp.dot(grad_query, w_query.T, preferred_element_type=jnp.float32) + jnp.dot(grad_rq, w_ret_query.T, preferred_element_type=jnp.float32) + jnp.dot(grad_rk, w_ret_key.T, preferred_element_type=jnp.float32) + jnp.dot(grad_rv, w_ret_value.T, preferred_element_type=jnp.float32)).astype(jnp.bfloat16)
        slot_rows = store[ids].reshape(-1, width)
        carry = carry + jnp.dot(slot_rows.T, grad_keys.reshape(-1, kv_width), preferred_element_type=jnp.float32)
        return (carry, (grad_rows_out, grad_keys, grad_values))
    start = jnp.zeros((width, kv_width), jnp.float32)
    key_weight_grad, outputs = lax.scan(per_sequence, start, (seq_tokens, seq_ids, seq_grad))
    grad_rows_all, slot_keys, slot_values = outputs
    flat_ids = passage_ids.reshape(-1).astype(jnp.int32)
    passage_keys = jax.ops.segment_sum(slot_keys.reshape(-1, plen * kv_width).astype(jnp.float32), flat_ids, num_segments=count)
    passage_values = jax.ops.segment_sum(slot_values.reshape(-1, plen * kv_width).astype(jnp.float32), flat_ids, num_segments=count)
    keys_bf = passage_keys.astype(jnp.bfloat16).reshape(count * plen, kv_width)
    values_bf = passage_values.astype(jnp.bfloat16).reshape(count * plen, kv_width)
    grad_store = (jnp.dot(keys_bf, w_key.T, preferred_element_type=jnp.float32) + jnp.dot(values_bf, w_value.T, preferred_element_type=jnp.float32)).astype(jnp.bfloat16).reshape(count, plen, width)
    return (grad_rows_all.reshape(-1, width), grad_store, key_weight_grad)
```

```python
import functools

import jax
import jax.numpy as jnp
from jax import lax
from jax.experimental import pallas as pl
from jax.experimental.pallas import tpu as pltpu
from jax.sharding import PartitionSpec as P

HEAD = 256
BLK = 64
KP = 4
MOST = 1


EPSILON = 1.0


def retention_grads(query_rows, key_rows, value_rows, rates, gains, cotangent):
    length = query_rows.shape[0]
    heads = rates.shape[0]
    queries = query_rows.reshape(length, heads, -1)
    keyset = key_rows.reshape(length, heads, -1)
    values = value_rows.reshape(length, heads, -1)
    positions = jnp.arange(length, dtype=jnp.float32)
    distance = positions[:, None] - positions[None, :]
    damping = jnp.where(
        distance >= 0.0, jnp.exp(-rates[:, None, None] * jnp.maximum(distance, 0.0)), 0.0
    ) * queries.shape[-1] ** (-0.5)
    raw = jnp.einsum("thd,shd->hts", queries, keyset, preferred_element_type=jnp.float32)
    weights = (raw * damping).astype(jnp.bfloat16)
    mixed = jnp.einsum("hts,she->the", weights, values, preferred_element_type=jnp.float32)
    inverse = lax.rsqrt(jnp.mean(mixed * mixed, axis=-1, keepdims=True) + EPSILON)
    scaled = cotangent.astype(jnp.float32).reshape(length, heads, -1) * gains.reshape(heads, -1)
    inner = jnp.mean(scaled * mixed, axis=-1, keepdims=True)
    grad_mixed = (inverse * scaled - inverse * inverse * inverse * mixed * inner).astype(
        jnp.bfloat16
    )
    grad_weights = (
        jnp.einsum("the,she->hts", grad_mixed, values, preferred_element_type=jnp.float32) * damping
    ).astype(jnp.bfloat16)
    grad_first = (
        jnp.einsum("hts,shd->thd", grad_weights, keyset, preferred_element_type=jnp.float32)
        .astype(jnp.bfloat16)
        .reshape(length, -1)
    )
    grad_second = (
        jnp.einsum("hts,thd->shd", grad_weights, queries, preferred_element_type=jnp.float32)
        .astype(jnp.bfloat16)
        .reshape(length, -1)
    )
    grad_third = (
        jnp.einsum("hts,the->she", weights, grad_mixed, preferred_element_type=jnp.float32)
        .astype(jnp.bfloat16)
        .reshape(length, -1)
    )
    return (grad_first, grad_second, grad_third)


def against_rows(left, weight):
    return lax.dot_general(
        left, weight, (((1,), (1,)), ((), ())), preferred_element_type=jnp.float32
    )


def across_rows(left, right):
    return lax.dot_general(
        left, right, (((0,), (0,)), ((), ())), preferred_element_type=jnp.float32
    )


def per_device_plain(
    tokens,
    store,
    passage_ids,
    w_query,
    w_key,
    w_value,
    w_ret_query,
    w_ret_key,
    w_ret_value,
    ret_rate,
    ret_gain,
    gate_logit,
    out_grad,
):
    owners = lax.axis_size("st")
    pass_dev, plen, width = store.shape
    length = tokens.shape[0]
    kv_width = w_key.shape[1]
    kv_local = kv_width // HEAD
    group = w_query.shape[1] // HEAD // kv_local
    blocks = length // BLK
    slot_ids = passage_ids.reshape(-1)
    slot_count = slot_ids.shape[0]
    slot_owner = slot_ids // pass_dev
    slot_local = slot_ids % pass_dev
    order = jnp.arange(slot_count, dtype=jnp.int32)
    same_owner = slot_owner[:, None] == slot_owner[None, :]
    rank = jnp.sum(same_owner & (order[None, :] < order[:, None]), axis=1)
    position = slot_owner * MOST + rank
    cells = owners * MOST
    placed = jnp.arange(cells, dtype=jnp.int32)[:, None] == position[None, :]
    request = (jnp.sum(jnp.where(placed, slot_local[None, :] + 1, 0), axis=1) - 1).reshape(
        owners, MOST
    )
    incoming = lax.all_to_all(request, "st", split_axis=0, concat_axis=0, tiled=True)
    wanted = incoming.reshape(-1)
    valid = wanted >= 0
    safe = jnp.maximum(wanted, 0)
    placed_bf = placed.astype(jnp.bfloat16)
    store_rows = store.reshape(-1, width)
    nothing = jnp.zeros((), jnp.bfloat16)
    own_kv = jnp.concatenate(
        [
            jnp.dot(store_rows, w_key, preferred_element_type=jnp.float32).astype(jnp.bfloat16),
            jnp.dot(store_rows, w_value, preferred_element_type=jnp.float32).astype(jnp.bfloat16),
        ],
        axis=1,
    ).reshape(pass_dev, plen, 2 * kv_width)
    reply = jnp.where(valid[:, None, None], own_kv[safe], nothing).reshape(
        owners, MOST, plen, 2 * kv_width
    )
    arrived = lax.all_to_all(reply, "st", split_axis=0, concat_axis=0, tiled=True)
    slot_kv = (
        across_rows(placed_bf, arrived.reshape(cells, -1))
        .astype(jnp.bfloat16)
        .reshape(slot_count, plen, 2 * kv_width)
    )
    factor = HEAD ** (-0.5)
    gate = jax.nn.sigmoid(gate_logit)
    query_bf = jnp.dot(tokens, w_query, preferred_element_type=jnp.float32).astype(jnp.bfloat16)
    queries = query_bf.reshape(blocks, BLK, kv_local, group, HEAD)
    keys = slot_kv[:, :, :kv_width].reshape(blocks, KP * plen, kv_local, HEAD)
    values = slot_kv[:, :, kv_width:].reshape(blocks, KP * plen, kv_local, HEAD)
    scores = (
        jnp.einsum("btkgd,bskd->bkgts", queries, keys, preferred_element_type=jnp.float32) * factor
    )
    expo = jnp.exp(scores)
    probs = expo / jnp.sum(expo, axis=-1, keepdims=True)
    probs_bf = probs.astype(jnp.bfloat16)
    attn = jnp.einsum("bkgts,bskd->btkgd", probs_bf, values, preferred_element_type=jnp.float32)
    grad_attn = out_grad.astype(jnp.float32).reshape(
        blocks, BLK, kv_local, group, HEAD
    ) * gate.reshape(kv_local, group, HEAD)
    grad_attn_bf = grad_attn.astype(jnp.bfloat16)
    grad_probs = jnp.einsum(
        "btkgd,bskd->bkgts", grad_attn_bf, values, preferred_element_type=jnp.float32
    )
    delta = jnp.moveaxis(jnp.sum(grad_attn * attn, axis=-1), 1, 3)
    grad_scores = (probs * (grad_probs - delta[..., None]) * factor).astype(jnp.bfloat16)
    grad_query = (
        jnp.einsum("bkgts,bskd->btkgd", grad_scores, keys, preferred_element_type=jnp.float32)
        .astype(jnp.bfloat16)
        .reshape(length, -1)
    )
    grad_keys = (
        jnp.einsum("bkgts,btkgd->bskd", grad_scores, queries, preferred_element_type=jnp.float32)
        .astype(jnp.bfloat16)
        .reshape(slot_count, plen, kv_width)
    )
    grad_values = (
        jnp.einsum("bkgts,btkgd->bskd", probs_bf, grad_attn_bf, preferred_element_type=jnp.float32)
        .astype(jnp.bfloat16)
        .reshape(slot_count, plen, kv_width)
    )
    slot_grad = jnp.concatenate([grad_keys, grad_values], axis=2)
    outgoing = (
        jnp.dot(placed_bf, slot_grad.reshape(slot_count, -1), preferred_element_type=jnp.float32)
        .astype(jnp.bfloat16)
        .reshape(owners, MOST, plen, 2 * kv_width)
    )
    returned = lax.all_to_all(outgoing, "st", split_axis=0, concat_axis=0, tiled=True)
    matched = (jnp.arange(pass_dev, dtype=jnp.int32)[:, None] == wanted[None, :]).astype(
        jnp.bfloat16
    )
    passage_grad = jnp.dot(
        matched, returned.reshape(cells, -1), preferred_element_type=jnp.float32
    ).reshape(pass_dev * plen, 2 * kv_width)
    key_grad = passage_grad[:, :kv_width]
    upper = key_grad.astype(jnp.bfloat16)
    lower = (key_grad - upper.astype(jnp.float32)).astype(jnp.bfloat16)
    key_term = across_rows(store_rows, upper) + across_rows(store_rows, lower)
    grad_key_weight = lax.psum(key_term, "st")
    passage_bf = passage_grad.astype(jnp.bfloat16)
    grad_store = lax.psum_scatter(
        (
            against_rows(passage_bf[:, :kv_width], w_key)
            + against_rows(passage_bf[:, kv_width:], w_value)
        ).astype(jnp.bfloat16),
        "tp",
        scatter_dimension=0,
        tiled=True,
    ).astype(jnp.float32)
    grad_store = grad_store.astype(jnp.bfloat16).reshape(-1, plen, width)
    ret_query = jnp.dot(tokens, w_ret_query, preferred_element_type=jnp.float32).astype(
        jnp.bfloat16
    )
    ret_key = jnp.dot(tokens, w_ret_key, preferred_element_type=jnp.float32).astype(jnp.bfloat16)
    ret_value = jnp.dot(tokens, w_ret_value, preferred_element_type=jnp.float32).astype(
        jnp.bfloat16
    )
    grad_rq, grad_rk, grad_rv = retention_grads(
        ret_query, ret_key, ret_value, ret_rate, ret_gain, out_grad
    )
    total = against_rows(grad_query, w_query)
    total = total + against_rows(grad_rq, w_ret_query)
    total = total + against_rows(grad_rk, w_ret_key)
    grad_tokens = lax.psum_scatter(
        (total + against_rows(grad_rv, w_ret_value)).astype(jnp.bfloat16),
        "tp",
        scatter_dimension=0,
        tiled=True,
    )
    return (grad_tokens, grad_store, grad_key_weight)


PLANE = 4
PARTS = 2
SPAN = 128
TILE = 256
BF = jnp.bfloat16
F32 = jnp.float32
MESH = pl.DeviceIdType.MESH


def nn(a, b):
    return lax.dot_general(a, b, (((1,), (0,)), ((), ())), preferred_element_type=F32)


def nt(a, b):
    return lax.dot_general(a, b, (((1,), (1,)), ((), ())), preferred_element_type=F32)


def tn(a, b):
    return lax.dot_general(a, b, (((0,), (0,)), ((), ())), preferred_element_type=F32)


def fused_kernel(
    n,
    ids_ref,
    rate_ref,
    gain_ref,
    gate_ref,
    tokens_hbm,
    store_hbm,
    wq_hbm,
    wk_hbm,
    wv_hbm,
    wrq_hbm,
    wrk_hbm,
    wrv_hbm,
    og_hbm,
    gt_hbm,
    gs_hbm,
    gkw_hbm,
    tokens,
    store,
    wq,
    wk,
    wv,
    wrq,
    wrk,
    wrv,
    og,
    q,
    rq,
    rk,
    rv,
    gq,
    grq,
    grk,
    grv,
    total,
    gt,
    gt_in,
    gs,
    gs_in,
    kv_col,
    kv_out,
    kv_in,
    req_out,
    req_in,
    stage_k,
    stage_v,
    gk_out,
    gv_out,
    gk_in,
    gv_in,
    pk,
    pv,
    slices,
    pk_in,
    p1_sum,
    p2_in,
    kg,
    owner_of,
    slot_of,
    local_of,
    load_sem,
    out_sem,
    tp_send,
    tp_recv,
    req_send,
    req_recv,
    gv_send,
    gv_recv,
    gk_send,
    gk_recv,
    z_send,
    z_recv,
    kv_send,
    kv_recv,
    rows_send,
    rows_recv,
    swap_send,
    swap_recv,
    pk_send,
    pk_recv,
    p2_send,
    p2_recv,
    p3_send,
    p3_recv,
    p4_send,
    p4_recv,
):
    me = lax.axis_index("st")
    tp = lax.axis_index("tp")
    length = tokens.shape[0]
    width = tokens.shape[1]
    plen = kv_in.shape[1]
    pass_dev = store.shape[0] // plen
    blocks = length // BLK
    slots = blocks * KP
    group = q.shape[1] // HEAD
    ret_heads = rate_ref.shape[0]
    depth = n // PLANE
    my_q = lax.rem(me, PLANE)
    my_z = lax.div(me, PLANE)
    half_tok = length // 2
    half_store = store.shape[0] // 2

    pairs = (
        (store_hbm, store),
        (wk_hbm, wk),
        (wv_hbm, wv),
        (tokens_hbm, tokens),
        (wrq_hbm, wrq),
        (wrk_hbm, wrk),
        (wrv_hbm, wrv),
        (og_hbm, og),
        (wq_hbm, wq),
    )
    loads = [pltpu.make_async_copy(a, b, load_sem.at[i]) for i, (a, b) in enumerate(pairs)]
    for load in loads[:3]:
        load.start()

    barrier = pltpu.get_barrier_semaphore()
    has_up = my_z < depth - 1
    has_down = my_z > 0

    def greet(axis, index):
        pl.semaphore_signal(barrier, inc=1, device_id={axis: index}, device_id_type=MESH)

    @pl.when(has_up)
    def _():
        greet("st", me + PLANE)

    @pl.when(has_down)
    def _():
        greet("st", me - PLANE)

    for i in range(1, PLANE):
        greet("st", my_z * PLANE + lax.rem(my_q + i, PLANE))
    greet("tp", 1 - tp)

    for s in range(slots):
        owner_of[s] = lax.div(ids_ref[s // KP, s % KP], pass_dev)

    def invert(o, carry):
        local = jnp.int32(0)
        where = jnp.int32(0)
        for s in range(slots):
            ident = ids_ref[s // KP, s % KP]
            hit = owner_of[s] == o
            local = jnp.where(hit, lax.rem(ident, pass_dev), local)
            where = jnp.where(hit, jnp.int32(s), where)
        slot_of[o] = where
        local_of[o] = local
        return carry

    lax.fori_loop(0, n, invert, 0)
    row_at = lax.broadcasted_iota(jnp.int32, req_out.shape[1:], 0)
    for c in range(PLANE):
        tile = jnp.zeros(req_out.shape[1:], jnp.int32)
        for z in range(depth):
            tile = jnp.where(row_at == z, local_of[z * PLANE + c], tile)
        req_out[c] = tile

    for load in loads[3:]:
        load.start()

    def peer(i):
        step = lax.div(i, PLANE)
        dz = jnp.where(my_z * 2 < depth, step, lax.rem(depth - step, depth))
        return lax.rem(my_z + dz, depth), lax.rem(my_q + lax.rem(i, PLANE), PLANE)

    def exchange(out_ref, in_ref, send, recv, i):
        z, c = peer(i)
        target = z * PLANE + c
        return pltpu.make_async_remote_copy(
            src_ref=out_ref.at[target],
            dst_ref=in_ref.at[me],
            send_sem=send.at[target],
            recv_sem=recv.at[me],
            device_id={"st": target},
            device_id_type=MESH,
        )

    def arrival(out_ref, in_ref, send, recv, i):
        z, c = peer(i)
        source = z * PLANE + c
        return pltpu.make_async_remote_copy(
            src_ref=out_ref.at[source],
            dst_ref=in_ref.at[source],
            send_sem=send.at[source],
            recv_sem=recv.at[source],
            device_id={"st": source},
            device_id_type=MESH,
        )

    def start_some(lo, hi, *refs):
        def body(i, carry):
            exchange(*refs, i).start()
            return carry

        lax.fori_loop(lo, hi, body, 0)

    def wait_recv_all(*refs):
        def body(i, carry):
            arrival(*refs, i).wait_recv()
            return carry

        lax.fori_loop(1, n, body, 0)

    def wait_send_all(*refs):
        def body(i, carry):
            exchange(*refs, i).wait_send()
            return carry

        lax.fori_loop(1, n, body, 0)

    def ask(i):
        z, c = peer(i)
        return pltpu.make_async_remote_copy(
            src_ref=req_out.at[c],
            dst_ref=req_in.at[me],
            send_sem=req_send.at[z * PLANE + c],
            recv_sem=req_recv.at[me],
            device_id={"st": z * PLANE + c},
            device_id_type=MESH,
        )

    def asked(i):
        z, c = peer(i)
        return pltpu.make_async_remote_copy(
            src_ref=req_out.at[c],
            dst_ref=req_in.at[z * PLANE + c],
            send_sem=req_send.at[z * PLANE + c],
            recv_sem=req_recv.at[z * PLANE + c],
            device_id={"st": z * PLANE + c},
            device_id_type=MESH,
        )

    gks = [
        (gk_out.at[c], gk_in.at[c], gk_send.at[c], gk_recv.at[c]) for c in range(PARTS)
    ]
    gvs = (gv_out, gv_in, gv_send, gv_recv)

    pl.semaphore_wait(
        barrier, PLANE + has_up.astype(jnp.int32) + has_down.astype(jnp.int32)
    )
    for i in range(1, PLANE):
        ask(i).start()
    req_in[me] = req_out[my_q]

    def along(up, z, p):
        at = kv_col.at[z, pl.ds(pl.multiple_of(p * plen, plen), plen)]
        return pltpu.make_async_remote_copy(
            src_ref=at,
            dst_ref=at,
            send_sem=z_send.at[up, z, p],
            recv_sem=z_recv.at[z, p],
            device_id={"st": me + (2 * up - 1) * PLANE},
            device_id_type=MESH,
        )

    for load in loads[:3]:
        load.wait()
    kv_col[my_z, :, :HEAD] = nn(store[...], wk[...]).astype(BF)
    kv_col[my_z, :, HEAD:] = nn(store[...], wv[...]).astype(BF)
    for p in range(pass_dev):

        @pl.when(has_up)
        def _():
            along(1, my_z, p).start()

        @pl.when(has_down)
        def _():
            along(0, my_z, p).start()

    def pump(k, p):
        @pl.when(my_z - k >= 0)
        def _():
            along(1, my_z - k, p).wait_recv()

            @pl.when(has_up)
            def _():
                along(1, my_z - k, p).start()

        @pl.when(my_z + k < depth)
        def _():
            along(0, my_z + k, p).wait_recv()

            @pl.when(has_down)
            def _():
                along(0, my_z + k, p).start()

    def names(row, p, lanes):
        mask = jnp.where(row == p, 1.0, 0.0).astype(F32)
        return jnp.concatenate([mask] * (lanes // mask.shape[1]), axis=1)

    def pick(row, z):
        chosen = jnp.zeros((plen, 2 * HEAD), F32)
        for p in range(pass_dev):
            chosen = chosen + names(row, p, 2 * HEAD) * kv_col[
                z, p * plen : (p + 1) * plen, :
            ].astype(F32)
        return chosen.astype(BF)

    def hand(z, i):
        return pltpu.make_async_remote_copy(
            src_ref=kv_out.at[z, i - 1],
            dst_ref=kv_in.at[z * PLANE + my_q],
            send_sem=kv_send.at[z, i - 1],
            recv_sem=kv_recv.at[z * PLANE + my_q],
            device_id={"st": my_z * PLANE + lax.rem(my_q + i, PLANE)},
            device_id_type=MESH,
        )

    def handed(z, i):
        owner = z * PLANE + lax.rem(my_q + i, PLANE)
        return pltpu.make_async_remote_copy(
            src_ref=kv_out.at[z, i - 1],
            dst_ref=kv_in.at[owner],
            send_sem=kv_send.at[z, i - 1],
            recv_sem=kv_recv.at[owner],
            device_id={"st": my_z * PLANE + lax.rem(my_q + i, PLANE)},
            device_id_type=MESH,
        )

    def spread(z):
        def body(i, carry):
            mate = my_z * PLANE + lax.rem(my_q + i, PLANE)
            kv_out[z, i - 1] = pick(req_in[mate, pl.ds(z, 1), :], z)
            hand(z, i).start()
            return carry

        lax.fori_loop(1, PLANE, body, 0)
        kv_in[z * PLANE + my_q] = pick(req_in[me, pl.ds(z, 1), :], z)

    def spread_round(k):
        def side(s, carry):
            z = my_z + k * (2 * s - 1)

            @pl.when((z >= 0) & (z < depth))
            def _():
                spread(z)

            return carry

        lax.fori_loop(0, 2, side, 0)

    quarter = width // PLANE
    share = quarter // 2

    def share_rows(i):
        other = lax.rem(my_q + i, PLANE)
        return pltpu.make_async_remote_copy(
            src_ref=store.at[:, pl.ds(pl.multiple_of(other * quarter + tp * share, share), share)],
            dst_ref=slices.at[i - 1, tp],
            send_sem=rows_send.at[i - 1],
            recv_sem=rows_recv.at[i - 1],
            device_id={"st": my_z * PLANE + other},
            device_id_type=MESH,
        )

    def swap_rows(i, part):
        return pltpu.make_async_remote_copy(
            src_ref=slices.at[i - 1, part],
            dst_ref=slices.at[i - 1, part],
            send_sem=swap_send.at[i - 1],
            recv_sem=swap_recv.at[i - 1],
            device_id={"tp": 1 - tp},
            device_id_type=MESH,
        )

    def project(w, out, then=None):
        def body(i, carry):
            cols = pl.ds(pl.multiple_of(i * TILE, TILE), TILE)
            out[:, cols] = nn(tokens[...], w[:, cols]).astype(BF)
            if then is not None:
                then(i)
            return carry

        lax.fori_loop(0, w.shape[1] // TILE, body, 0)

    loads[3].wait()
    for load, w, out in ((loads[4], wrq, rq), (loads[5], wrk, rk)):
        load.wait()
        project(w, out)
    for i in range(1, PLANE):
        asked(i).wait_recv()
    spread(my_z)
    for i in range(1, PLANE):
        share_rows(i).start()
    loads[6].wait()
    project(wrv, rv)
    loads[7].wait()

    ret_key = rq.shape[1] // ret_heads
    ret_value = rv.shape[1] // ret_heads
    at_t = lax.broadcasted_iota(jnp.int32, (length, length), 0)
    at_s = lax.broadcasted_iota(jnp.int32, (length, length), 1)
    distance = (at_t - at_s).astype(F32)

    def pump_part(k, i, count):
        each = pass_dev // count
        for p in range(each):
            pump(k, i * each + p)

    def retention(j, carry):
        kc = pl.ds(pl.multiple_of(j * ret_key, ret_key), ret_key)
        vc = pl.ds(pl.multiple_of(j * ret_value, ret_value), ret_value)
        damping = jnp.where(
            distance >= 0.0, jnp.exp(-rate_ref[j] * jnp.maximum(distance, 0.0)), 0.0
        ) * ret_key ** (-0.5)
        weights = (nt(rq[:, kc], rk[:, kc]) * damping).astype(BF)
        y = nn(weights, rv[:, vc])
        r = lax.rsqrt(jnp.mean(y * y, axis=1, keepdims=True) + EPSILON)
        c = og[:, vc].astype(F32) * gain_ref[:, vc]
        inner = jnp.mean(c * y, axis=1, keepdims=True)
        gy = (r * c - r * r * r * y * inner).astype(BF)
        gw = (nt(gy, rv[:, vc]) * damping).astype(BF)
        grq[:, kc] = nn(gw, rk[:, kc]).astype(BF)
        grk[:, kc] = tn(gw, rq[:, kc]).astype(BF)
        grv[:, vc] = tn(weights, gy).astype(BF)
        pump_part(1, j, ret_heads)
        return carry

    lax.fori_loop(0, ret_heads, retention, 0)
    spread_round(1)
    loads[8].wait()
    project(wq, q, lambda i: pump_part(2, i, wq.shape[1] // TILE))
    spread_round(2)

    def ret_total(i, carry):
        wide = width // pass_dev
        rows = pl.ds(pl.multiple_of(i * wide, wide), wide)
        total[:, rows] = (
            nt(grq[...], wrq[rows, :]) + nt(grk[...], wrk[rows, :]) + nt(grv[...], wrv[rows, :])
        )
        pump_part(3, i, pass_dev)
        return carry

    lax.fori_loop(0, pass_dev, ret_total, 0)
    spread_round(3)
    for i in range(1, PLANE):
        share_rows(i).wait_recv()
        swap_rows(i, tp).start()

    def wait_handed(z, carry):
        for i in range(1, PLANE):
            handed(z, i).wait_recv()
        return carry

    lax.fori_loop(0, depth, wait_handed, 0)

    def ask_far(i, carry):
        ask(i).start()
        return carry

    lax.fori_loop(PLANE, n, ask_far, 0)
    factor = HEAD ** (-0.5)

    def attend(b, carry):
        rows = pl.ds(pl.multiple_of(b * BLK, BLK), BLK)
        read = [kv_in[owner_of[b * KP + k]] for k in range(KP)]
        keys = jnp.concatenate([x[:, :HEAD] for x in read], axis=0)
        values = jnp.concatenate([x[:, HEAD:] for x in read], axis=0)
        cols = [slice(g * HEAD, (g + 1) * HEAD) for g in range(group)]
        queries = jnp.concatenate([q[rows, c] for c in cols], axis=0)
        expo = jnp.exp(nt(queries, keys) * factor)
        probs = expo / jnp.sum(expo, axis=1, keepdims=True)
        probs_bf = probs.astype(BF)
        attn = nn(probs_bf, values)
        grad_attn = jnp.concatenate(
            [
                og[rows, c].astype(F32) * (1.0 / (1.0 + jnp.exp(-gate_ref[:, c])))
                for c in cols
            ],
            axis=0,
        )
        grad_attn_bf = grad_attn.astype(BF)
        grad_probs = nt(grad_attn_bf, values)
        delta = jnp.sum(grad_attn * attn, axis=1, keepdims=True)
        scores = (probs * (grad_probs - delta) * factor).astype(BF)
        grad_query = nn(scores, keys).astype(BF)
        for g, c in enumerate(cols):
            gq[rows, c] = grad_query[g * BLK : (g + 1) * BLK, :]
        dk = tn(scores, queries).astype(BF)
        dv = tn(probs_bf, grad_attn_bf).astype(BF)
        for k in range(KP):
            for c in range(PARTS):
                stage_k[c, b * KP + k] = dk[k * plen : (k + 1) * plen, c * SPAN : (c + 1) * SPAN]
            stage_v[b * KP + k] = dv[k * plen : (k + 1) * plen, :]
        return carry

    lax.fori_loop(0, blocks, attend, 0)

    def place(stage, out):
        def body(o, carry):
            out[o] = stage[slot_of[o]]
            return carry

        lax.fori_loop(0, n, body, 0)

    for c in range(PARTS):
        place(stage_k.at[c], gk_out.at[c])
        start_some(1, n, *gks[c])
    place(stage_v, gv_out)
    for c in range(PARTS):
        gk_in[c, me] = gk_out[c, me]
    gv_in[me] = gv_out[me]

    def finish_total(i, carry):
        rows = pl.ds(pl.multiple_of(i * TILE, TILE), TILE)
        gt[:, rows] = (total[:, rows] + nt(gq[...], wq[rows, :])).astype(BF)
        return carry

    lax.fori_loop(0, width // TILE, finish_total, 0)

    def to_partner(out_ref, in_ref, half, at):
        return pltpu.make_async_remote_copy(
            src_ref=out_ref.at[pl.ds(pl.multiple_of((1 - tp) * half, half), half)],
            dst_ref=in_ref,
            send_sem=tp_send.at[at],
            recv_sem=tp_recv.at[at],
            device_id={"tp": 1 - tp},
            device_id_type=MESH,
        )

    def add_own(out_ref, in_ref, half):
        own = out_ref[pl.ds(pl.multiple_of(tp * half, half), half), :]
        in_ref[...] = (own.astype(F32) + in_ref[...].astype(F32)).astype(BF)

    token_swap = to_partner(gt, gt_in, half_tok, 0)
    token_swap.start()

    def gather_sum(in_ref, out_ref):
        lanes = out_ref.shape[1]
        for p in range(pass_dev):

            def body(r, acc):
                row = req_in[r, pl.ds(my_z, 1), :]
                return acc + names(row, p, lanes) * in_ref[r].astype(F32)

            acc = lax.fori_loop(0, n, body, jnp.zeros((plen, lanes), F32))
            out_ref[p * plen : (p + 1) * plen, :] = acc.astype(BF)

    def share_key(c, i):
        return pltpu.make_async_remote_copy(
            src_ref=pk.at[c],
            dst_ref=pk_in.at[c, i - 1],
            send_sem=pk_send.at[c, i - 1],
            recv_sem=pk_recv.at[c, i - 1],
            device_id={"st": my_z * PLANE + lax.rem(my_q + i, PLANE)},
            device_id_type=MESH,
        )

    def column_reduce(c, i):
        other = lax.rem(my_z + i, depth)
        return pltpu.make_async_remote_copy(
            src_ref=p1_sum.at[c, other],
            dst_ref=p2_in.at[c, i - 1],
            send_sem=p2_send.at[c, i - 1],
            recv_sem=p2_recv.at[c, i - 1],
            device_id={"st": other * PLANE + my_q},
            device_id_type=MESH,
        )

    def column_gather(c, i, source):
        at = kg.at[c, my_q * depth + source]
        return pltpu.make_async_remote_copy(
            src_ref=at,
            dst_ref=at,
            send_sem=p3_send.at[c, i - 1],
            recv_sem=p3_recv.at[c, i - 1],
            device_id={"st": lax.rem(my_z + i, depth) * PLANE + my_q},
            device_id_type=MESH,
        )

    def plane_gather(c, i, source, z):
        at = kg.at[c, source * depth + z]
        return pltpu.make_async_remote_copy(
            src_ref=at,
            dst_ref=at,
            send_sem=p4_send.at[c, z, i - 1],
            recv_sem=p4_recv.at[c, z, i - 1],
            device_id={"st": my_z * PLANE + lax.rem(my_q + i, PLANE)},
            device_id_type=MESH,
        )

    for i in range(1, PLANE):
        swap_rows(i, 1 - tp).wait_recv()

    def asked_far(i, carry):
        asked(i).wait_recv()
        return carry

    lax.fori_loop(PLANE, n, asked_far, 0)

    own_cols = pl.ds(pl.multiple_of(my_q * quarter, quarter), quarter)
    own_terms = []
    for c in range(PARTS):
        wait_recv_all(*gks[c])
        gather_sum(gk_in.at[c], pk.at[c])
        for i in range(1, PLANE):
            share_key(c, i).start()
        own_terms.append(tn(store[:, own_cols], pk[c]))
        if c == 0:
            start_some(PLANE, 2 * PLANE, *gvs)

    token_swap.wait_recv()
    add_own(gt, gt_in, half_tok)
    token_out = pltpu.make_async_copy(gt_in, gt_hbm, out_sem.at[0])
    token_out.start()

    for c in range(PARTS):
        for i in range(1, PLANE):
            share_key(c, i).wait_recv()
        for part in range(2):
            acc = own_terms[c][part * share : (part + 1) * share]
            for i in range(1, PLANE):
                acc = acc + tn(slices[i - 1, part], pk_in[c, i - 1])
            acc = acc.reshape(depth // 2, -1, SPAN)
            p1_sum[c, part * depth // 2 : (part + 1) * depth // 2] = acc.astype(BF)
        for i in range(1, depth):
            column_reduce(c, i).start()
        start_some((c + 2) * PLANE, (c + 3) * PLANE, *gvs)

    for c in range(PARTS):
        for i in range(1, depth):
            column_reduce(c, i).wait_recv()
        acc = p1_sum[c, my_z].astype(F32)
        for i in range(1, depth):
            acc = acc + p2_in[c, i - 1].astype(F32)
        kg[c, my_q * depth + my_z] = acc.astype(BF)
        for i in range(1, depth):
            column_gather(c, i, my_z).start()
        for i in range(1, PLANE):
            plane_gather(c, i, my_q, my_z).start()
    start_some(1, PLANE, *gvs)

    for c in range(PARTS):
        for s in range(1, depth):
            i = jnp.where(my_z * 2 < depth, depth - s, s)
            source = lax.rem(my_z + depth - i, depth)
            column_gather(c, i, source).wait_recv()
            for j in range(1, PLANE):
                plane_gather(c, j, my_q, source).start()

    wait_recv_all(*gvs)
    gather_sum(gv_in, pv)

    def store_grad(i, carry):
        rows = pl.ds(pl.multiple_of(i * TILE, TILE), TILE)
        keys = jnp.concatenate([pk[c] for c in range(PARTS)], axis=1)
        gs[:, rows] = (nt(keys, wk[rows, :]) + nt(pv[...], wv[rows, :])).astype(BF)
        return carry

    lax.fori_loop(0, width // TILE, store_grad, 0)
    store_swap = to_partner(gs, gs_in, half_store, 1)
    store_swap.start()
    store_swap.wait_recv()
    add_own(gs, gs_in, half_store)
    store_out = pltpu.make_async_copy(gs_in, gs_hbm, out_sem.at[1])
    store_out.start()

    for c in range(PARTS):
        for z in range(depth):
            for i in range(1, PLANE):
                plane_gather(c, i, lax.rem(my_q + PLANE - i, PLANE), z).wait_recv()
    weight_out = pltpu.make_async_copy(kg, gkw_hbm, out_sem.at[2])
    weight_out.start()

    def ask_done(i, carry):
        ask(i).wait_send()
        return carry

    lax.fori_loop(1, n, ask_done, 0)

    def along_done(z, carry):
        for p in range(pass_dev):

            @pl.when(has_up & (z <= my_z))
            def _():
                along(1, z, p).wait_send()

            @pl.when(has_down & (z >= my_z))
            def _():
                along(0, z, p).wait_send()

        for i in range(1, PLANE):
            hand(z, i).wait_send()
        return carry

    lax.fori_loop(0, depth, along_done, 0)
    wait_send_all(*gvs)
    token_swap.wait_send()
    store_swap.wait_send()
    for c in range(PARTS):
        wait_send_all(*gks[c])
        for i in range(1, PLANE):
            share_key(c, i).wait_send()
            for z in range(depth):
                plane_gather(c, i, my_q, z).wait_send()
        for i in range(1, depth):
            column_reduce(c, i).wait_send()
            column_gather(c, i, my_z).wait_send()
    for i in range(1, PLANE):
        share_rows(i).wait_send()
        swap_rows(i, tp).wait_send()
    token_out.wait()
    store_out.wait()
    weight_out.wait()


def finish_kernel(gt_hbm, gs_hbm, kg_hbm, ot_hbm, os_hbm, ok_hbm, gt, gs, kg, out, in_sem, out_sem):
    loads = [
        pltpu.make_async_copy(a, b, in_sem.at[i])
        for i, (a, b) in enumerate(((kg_hbm.at[0], kg.at[0]), (kg_hbm.at[1], kg.at[1]), (gt_hbm, gt), (gs_hbm, gs)))
    ]
    for load in loads:
        load.start()
    for c in range(PARTS):
        loads[c].wait()
        out[:, c * SPAN : (c + 1) * SPAN] = kg[c].astype(F32)
    stores = [pltpu.make_async_copy(out, ok_hbm, out_sem.at[0])]
    stores[0].start()
    for i, (a, b) in enumerate(((gt, ot_hbm), (gs, os_hbm))):
        loads[2 + i].wait()
        stores.append(pltpu.make_async_copy(a, b, out_sem.at[1 + i]))
        stores[-1].start()
    for store in stores:
        store.wait()


def per_device(sizes, *args):
    (tokens, store, ids, wq, wk, wv, wrq, wrk, wrv, rate, gain, gate, og) = args
    n = sizes["st"]
    pass_dev, plen, width = store.shape
    length = tokens.shape[0]
    rows = pass_dev * plen
    weight_cols = sum(w.shape[1] for w in (wq, wk, wv, wrq, wrk, wrv))
    fits = (
        sizes["tp"] == 2
        and wk.shape[1] == HEAD
        and HEAD == PARTS * SPAN
        and ids.size == n
        and n == PLANE * 4
        and pass_dev == 4
        and rate.shape[0] == 4
        and wq.shape[1] == 4 * TILE
        and width % (n * 128) == 0
        and width * weight_cols + n * plen * HEAD * 12 + length * width * 12 < 24 * 2**20
    )
    if not fits:
        return per_device_plain(*args)
    depth = n // PLANE
    piece = width // n

    def vm(*shape, dtype=BF):
        return pltpu.VMEM(shape, dtype)

    any_spec = pl.BlockSpec(memory_space=pl.ANY)
    smem = pl.BlockSpec(memory_space=pltpu.SMEM)
    vmem = pl.BlockSpec(memory_space=pltpu.VMEM)
    dma = pltpu.SemaphoreType.DMA
    like = [vm(*x.shape) for x in (tokens,)] + [vm(rows, width)]
    like += [vm(*x.shape) for x in (wq, wk, wv, wrq, wrk, wrv, og)]
    qs = [vm(length, w.shape[1]) for w in (wq, wrq, wrk, wrv)]
    scratch = (
        like
        + qs
        + qs
        + [
            vm(length, width, dtype=F32),
            vm(length, width),
            vm(length // 2, width),
            vm(rows, width),
            vm(rows // 2, width),
            vm(depth, rows, 2 * HEAD),
            vm(depth, PLANE - 1, plen, 2 * HEAD),
            vm(n, plen, 2 * HEAD),
            vm(PLANE, 8, 128, dtype=jnp.int32),
            vm(n, 8, 128, dtype=jnp.int32),
            vm(PARTS, n, plen, SPAN),
            vm(n, plen, HEAD),
            vm(PARTS, n, plen, SPAN),
            vm(n, plen, HEAD),
            vm(PARTS, n, plen, SPAN),
            vm(n, plen, HEAD),
            vm(PARTS, rows, SPAN),
            vm(rows, HEAD),
            vm(PLANE - 1, 2, rows, width // (2 * PLANE)),
            vm(PARTS, PLANE - 1, rows, SPAN),
            vm(PARTS, depth, piece, SPAN),
            vm(PARTS, depth - 1, piece, SPAN),
            vm(PARTS, n, piece, SPAN),
            pltpu.SMEM((n,), jnp.int32),
            pltpu.SMEM((n,), jnp.int32),
            pltpu.SMEM((n,), jnp.int32),
            dma((9,)),
            dma((3,)),
            dma((2,)),
            dma((2,)),
        ]
        + [dma((n,))] * 4
        + [dma((PARTS, n))] * 2
        + [dma((2, depth, pass_dev)), dma((depth, pass_dev))]
        + [dma((depth, PLANE - 1)), dma((n,))]
        + [dma((PLANE - 1,))] * 4
        + [dma((PARTS, PLANE - 1))] * 2
        + [dma((PARTS, depth - 1))] * 4
        + [dma((PARTS, depth, PLANE - 1))] * 2
    )
    grad_tokens, grad_store, grad_key = pl.pallas_call(
        functools.partial(fused_kernel, n),
        out_shape=(
            jax.ShapeDtypeStruct((length // 2, width), BF),
            jax.ShapeDtypeStruct((rows // 2, width), BF),
            jax.ShapeDtypeStruct((PARTS, n, piece, SPAN), BF),
        ),
        in_specs=[smem, smem, vmem, vmem] + [any_spec] * 9,
        out_specs=(any_spec, any_spec, any_spec),
        scratch_shapes=scratch,
        compiler_params=pltpu.CompilerParams(
            collective_id=0, has_side_effects=True, vmem_limit_bytes=60 * 2**20
        ),
    )(
        ids,
        rate,
        gain.reshape(1, -1),
        gate.reshape(1, -1),
        tokens,
        store.reshape(rows, width),
        wq,
        wk,
        wv,
        wrq,
        wrk,
        wrv,
        og,
    )
    grad_tokens, grad_store, grad_key = pl.pallas_call(
        finish_kernel,
        out_shape=(
            jax.ShapeDtypeStruct((length // 2, width), BF),
            jax.ShapeDtypeStruct((rows // 2, width), BF),
            jax.ShapeDtypeStruct((width, HEAD), F32),
        ),
        in_specs=[any_spec] * 3,
        out_specs=(any_spec, any_spec, any_spec),
        scratch_shapes=[
            vm(length // 2, width),
            vm(rows // 2, width),
            vm(PARTS, width, SPAN),
            vm(width, HEAD, dtype=F32),
            dma((4,)),
            dma((3,)),
        ],
    )(grad_tokens, grad_store, grad_key.reshape(PARTS, width, SPAN))
    return (grad_tokens, grad_store.reshape(pass_dev // 2, plen, width), grad_key)


def solution(mesh):
    return jax.shard_map(
        functools.partial(per_device, dict(mesh.shape)),
        mesh=mesh,
        in_specs=(
            P("st", None),
            P("st", None, None),
            P("st", None),
            P(None, "tp"),
            P(None, "tp"),
            P(None, "tp"),
            P(None, "tp"),
            P(None, "tp"),
            P(None, "tp"),
            P("tp"),
            P("tp"),
            P("tp"),
            P("st", "tp"),
        ),
        out_specs=(P(("st", "tp"), None), P(("st", "tp"), None, None), P(None, "tp")),
        check_vma=False,
    )
```

```python
import functools

import jax
import jax.numpy as jnp
from jax import lax
from jax.experimental import pallas as pl
from jax.experimental.pallas import tpu as pltpu
from jax.sharding import PartitionSpec as P

HEAD = 256
BLK = 64
KP = 4
MOST = 1


EPSILON = 1.0


def retention_grads(query_rows, key_rows, value_rows, rates, gains, cotangent):
    length = query_rows.shape[0]
    heads = rates.shape[0]
    queries = query_rows.reshape(length, heads, -1)
    keyset = key_rows.reshape(length, heads, -1)
    values = value_rows.reshape(length, heads, -1)
    positions = jnp.arange(length, dtype=jnp.float32)
    distance = positions[:, None] - positions[None, :]
    damping = jnp.where(
        distance >= 0.0, jnp.exp(-rates[:, None, None] * jnp.maximum(distance, 0.0)), 0.0
    ) * queries.shape[-1] ** (-0.5)
    raw = jnp.einsum("thd,shd->hts", queries, keyset, preferred_element_type=jnp.float32)
    weights = (raw * damping).astype(jnp.bfloat16)
    mixed = jnp.einsum("hts,she->the", weights, values, preferred_element_type=jnp.float32)
    inverse = lax.rsqrt(jnp.mean(mixed * mixed, axis=-1, keepdims=True) + EPSILON)
    scaled = cotangent.astype(jnp.float32).reshape(length, heads, -1) * gains.reshape(heads, -1)
    inner = jnp.mean(scaled * mixed, axis=-1, keepdims=True)
    grad_mixed = (inverse * scaled - inverse * inverse * inverse * mixed * inner).astype(
        jnp.bfloat16
    )
    grad_weights = (
        jnp.einsum("the,she->hts", grad_mixed, values, preferred_element_type=jnp.float32) * damping
    ).astype(jnp.bfloat16)
    grad_first = (
        jnp.einsum("hts,shd->thd", grad_weights, keyset, preferred_element_type=jnp.float32)
        .astype(jnp.bfloat16)
        .reshape(length, -1)
    )
    grad_second = (
        jnp.einsum("hts,thd->shd", grad_weights, queries, preferred_element_type=jnp.float32)
        .astype(jnp.bfloat16)
        .reshape(length, -1)
    )
    grad_third = (
        jnp.einsum("hts,the->she", weights, grad_mixed, preferred_element_type=jnp.float32)
        .astype(jnp.bfloat16)
        .reshape(length, -1)
    )
    return (grad_first, grad_second, grad_third)


def against_rows(left, weight):
    return lax.dot_general(
        left, weight, (((1,), (1,)), ((), ())), preferred_element_type=jnp.float32
    )


def across_rows(left, right):
    return lax.dot_general(
        left, right, (((0,), (0,)), ((), ())), preferred_element_type=jnp.float32
    )


def per_device_plain(
    tokens,
    store,
    passage_ids,
    w_query,
    w_key,
    w_value,
    w_ret_query,
    w_ret_key,
    w_ret_value,
    ret_rate,
    ret_gain,
    gate_logit,
    out_grad,
):
    owners = lax.axis_size("st")
    pass_dev, plen, width = store.shape
    length = tokens.shape[0]
    kv_width = w_key.shape[1]
    kv_local = kv_width // HEAD
    group = w_query.shape[1] // HEAD // kv_local
    blocks = length // BLK
    slot_ids = passage_ids.reshape(-1)
    slot_count = slot_ids.shape[0]
    slot_owner = slot_ids // pass_dev
    slot_local = slot_ids % pass_dev
    order = jnp.arange(slot_count, dtype=jnp.int32)
    same_owner = slot_owner[:, None] == slot_owner[None, :]
    rank = jnp.sum(same_owner & (order[None, :] < order[:, None]), axis=1)
    position = slot_owner * MOST + rank
    cells = owners * MOST
    placed = jnp.arange(cells, dtype=jnp.int32)[:, None] == position[None, :]
    request = (jnp.sum(jnp.where(placed, slot_local[None, :] + 1, 0), axis=1) - 1).reshape(
        owners, MOST
    )
    incoming = lax.all_to_all(request, "st", split_axis=0, concat_axis=0, tiled=True)
    wanted = incoming.reshape(-1)
    valid = wanted >= 0
    safe = jnp.maximum(wanted, 0)
    placed_bf = placed.astype(jnp.bfloat16)
    store_rows = store.reshape(-1, width)
    nothing = jnp.zeros((), jnp.bfloat16)
    own_kv = jnp.concatenate(
        [
            jnp.dot(store_rows, w_key, preferred_element_type=jnp.float32).astype(jnp.bfloat16),
            jnp.dot(store_rows, w_value, preferred_element_type=jnp.float32).astype(jnp.bfloat16),
        ],
        axis=1,
    ).reshape(pass_dev, plen, 2 * kv_width)
    reply = jnp.where(valid[:, None, None], own_kv[safe], nothing).reshape(
        owners, MOST, plen, 2 * kv_width
    )
    arrived = lax.all_to_all(reply, "st", split_axis=0, concat_axis=0, tiled=True)
    slot_kv = (
        across_rows(placed_bf, arrived.reshape(cells, -1))
        .astype(jnp.bfloat16)
        .reshape(slot_count, plen, 2 * kv_width)
    )
    factor = HEAD ** (-0.5)
    gate = jax.nn.sigmoid(gate_logit)
    query_bf = jnp.dot(tokens, w_query, preferred_element_type=jnp.float32).astype(jnp.bfloat16)
    queries = query_bf.reshape(blocks, BLK, kv_local, group, HEAD)
    keys = slot_kv[:, :, :kv_width].reshape(blocks, KP * plen, kv_local, HEAD)
    values = slot_kv[:, :, kv_width:].reshape(blocks, KP * plen, kv_local, HEAD)
    scores = (
        jnp.einsum("btkgd,bskd->bkgts", queries, keys, preferred_element_type=jnp.float32) * factor
    )
    expo = jnp.exp(scores)
    probs = expo / jnp.sum(expo, axis=-1, keepdims=True)
    probs_bf = probs.astype(jnp.bfloat16)
    attn = jnp.einsum("bkgts,bskd->btkgd", probs_bf, values, preferred_element_type=jnp.float32)
    grad_attn = out_grad.astype(jnp.float32).reshape(
        blocks, BLK, kv_local, group, HEAD
    ) * gate.reshape(kv_local, group, HEAD)
    grad_attn_bf = grad_attn.astype(jnp.bfloat16)
    grad_probs = jnp.einsum(
        "btkgd,bskd->bkgts", grad_attn_bf, values, preferred_element_type=jnp.float32
    )
    delta = jnp.moveaxis(jnp.sum(grad_attn * attn, axis=-1), 1, 3)
    grad_scores = (probs * (grad_probs - delta[..., None]) * factor).astype(jnp.bfloat16)
    grad_query = (
        jnp.einsum("bkgts,bskd->btkgd", grad_scores, keys, preferred_element_type=jnp.float32)
        .astype(jnp.bfloat16)
        .reshape(length, -1)
    )
    grad_keys = (
        jnp.einsum("bkgts,btkgd->bskd", grad_scores, queries, preferred_element_type=jnp.float32)
        .astype(jnp.bfloat16)
        .reshape(slot_count, plen, kv_width)
    )
    grad_values = (
        jnp.einsum("bkgts,btkgd->bskd", probs_bf, grad_attn_bf, preferred_element_type=jnp.float32)
        .astype(jnp.bfloat16)
        .reshape(slot_count, plen, kv_width)
    )
    slot_grad = jnp.concatenate([grad_keys, grad_values], axis=2)
    outgoing = (
        jnp.dot(placed_bf, slot_grad.reshape(slot_count, -1), preferred_element_type=jnp.float32)
        .astype(jnp.bfloat16)
        .reshape(owners, MOST, plen, 2 * kv_width)
    )
    returned = lax.all_to_all(outgoing, "st", split_axis=0, concat_axis=0, tiled=True)
    matched = (jnp.arange(pass_dev, dtype=jnp.int32)[:, None] == wanted[None, :]).astype(
        jnp.bfloat16
    )
    passage_grad = jnp.dot(
        matched, returned.reshape(cells, -1), preferred_element_type=jnp.float32
    ).reshape(pass_dev * plen, 2 * kv_width)
    key_grad = passage_grad[:, :kv_width]
    upper = key_grad.astype(jnp.bfloat16)
    lower = (key_grad - upper.astype(jnp.float32)).astype(jnp.bfloat16)
    key_term = across_rows(store_rows, upper) + across_rows(store_rows, lower)
    grad_key_weight = lax.psum(key_term, "st")
    passage_bf = passage_grad.astype(jnp.bfloat16)
    grad_store = lax.psum_scatter(
        (
            against_rows(passage_bf[:, :kv_width], w_key)
            + against_rows(passage_bf[:, kv_width:], w_value)
        ).astype(jnp.bfloat16),
        "tp",
        scatter_dimension=0,
        tiled=True,
    ).astype(jnp.float32)
    grad_store = grad_store.astype(jnp.bfloat16).reshape(-1, plen, width)
    ret_query = jnp.dot(tokens, w_ret_query, preferred_element_type=jnp.float32).astype(
        jnp.bfloat16
    )
    ret_key = jnp.dot(tokens, w_ret_key, preferred_element_type=jnp.float32).astype(jnp.bfloat16)
    ret_value = jnp.dot(tokens, w_ret_value, preferred_element_type=jnp.float32).astype(
        jnp.bfloat16
    )
    grad_rq, grad_rk, grad_rv = retention_grads(
        ret_query, ret_key, ret_value, ret_rate, ret_gain, out_grad
    )
    total = against_rows(grad_query, w_query)
    total = total + against_rows(grad_rq, w_ret_query)
    total = total + against_rows(grad_rk, w_ret_key)
    grad_tokens = lax.psum_scatter(
        (total + against_rows(grad_rv, w_ret_value)).astype(jnp.bfloat16),
        "tp",
        scatter_dimension=0,
        tiled=True,
    )
    return (grad_tokens, grad_store, grad_key_weight)


PLANE = 4
PARTS = 2
SPAN = 128
CHUNKS = 4
SWAPS = 4
TOGETHER = 2
TILE = 256
BF = jnp.bfloat16
F32 = jnp.float32
MESH = pl.DeviceIdType.MESH


def nn(a, b):
    return lax.dot_general(a, b, (((1,), (0,)), ((), ())), preferred_element_type=F32)


def nt(a, b):
    return lax.dot_general(a, b, (((1,), (1,)), ((), ())), preferred_element_type=F32)


def tn(a, b):
    return lax.dot_general(a, b, (((0,), (0,)), ((), ())), preferred_element_type=F32)


def fused_kernel(
    n,
    ids_ref,
    rate_ref,
    gain_ref,
    gate_ref,
    tokens_hbm,
    store_hbm,
    wq_hbm,
    wk_hbm,
    wv_hbm,
    wrq_hbm,
    wrk_hbm,
    wrv_hbm,
    og_hbm,
    gt_hbm,
    gs_hbm,
    gkw_hbm,
    tokens,
    store,
    wq,
    wk,
    wv,
    wrq,
    wrk,
    wrv,
    og,
    q,
    rq,
    rk,
    rv,
    gq,
    grq,
    grk,
    grv,
    total,
    gt,
    gt_in,
    gs_key,
    gs,
    gs_in,
    ga,
    ga_bf,
    kv_col,
    kv_out,
    kv_in,
    req_out,
    req_in,
    stage_k,
    stage_v,
    gk_out,
    gv_out,
    gk_in,
    v_in,
    vp_out,
    v_mid,
    v_add,
    pk,
    pv,
    slices,
    pk_in,
    p1_sum,
    p2_in,
    kg,
    owner_of,
    slot_of,
    local_of,
    load_sem,
    out_sem,
    tp_send,
    tp_recv,
    req_send,
    req_recv,
    v_send,
    v_recv,
    vp_send,
    vp_recv,
    gk_send,
    gk_recv,
    z_send,
    z_recv,
    kv_send,
    kv_recv,
    rows_send,
    rows_recv,
    swap_send,
    swap_recv,
    pk_send,
    pk_recv,
    p2_send,
    p2_recv,
    p3_send,
    p3_recv,
    p4_send,
    p4_recv,
):
    me = lax.axis_index("st")
    tp = lax.axis_index("tp")
    length = tokens.shape[0]
    width = tokens.shape[1]
    plen = kv_in.shape[1]
    pass_dev = store.shape[0] // plen
    blocks = length // BLK
    slots = blocks * KP
    group = q.shape[1] // HEAD
    ret_heads = rate_ref.shape[0]
    depth = n // PLANE
    my_q = lax.rem(me, PLANE)
    my_z = lax.div(me, PLANE)
    half_tok = length // 2
    half_store = store.shape[0] // 2

    pairs = (
        (store_hbm, store),
        (wk_hbm, wk),
        (wv_hbm, wv),
        (tokens_hbm, tokens),
        (wrq_hbm, wrq),
        (wrk_hbm, wrk),
        (wrv_hbm, wrv),
        (og_hbm, og),
        (wq_hbm, wq),
    )
    loads = [pltpu.make_async_copy(a, b, load_sem.at[i]) for i, (a, b) in enumerate(pairs)]
    for load in loads[:3]:
        load.start()

    barrier = pltpu.get_barrier_semaphore()
    has_up = my_z < depth - 1
    has_down = my_z > 0

    def greet(axis, index):
        pl.semaphore_signal(barrier, inc=1, device_id={axis: index}, device_id_type=MESH)

    @pl.when(has_up)
    def _():
        greet("st", me + PLANE)

    @pl.when(has_down)
    def _():
        greet("st", me - PLANE)

    for i in range(1, PLANE):
        greet("st", my_z * PLANE + lax.rem(my_q + i, PLANE))
    greet("tp", 1 - tp)

    for s in range(slots):
        owner_of[s] = lax.div(ids_ref[s // KP, s % KP], pass_dev)

    def invert(o, carry):
        local = jnp.int32(0)
        where = jnp.int32(0)
        for s in range(slots):
            ident = ids_ref[s // KP, s % KP]
            hit = owner_of[s] == o
            local = jnp.where(hit, lax.rem(ident, pass_dev), local)
            where = jnp.where(hit, jnp.int32(s), where)
        slot_of[o] = where
        local_of[o] = local
        return carry

    lax.fori_loop(0, n, invert, 0)
    row_at = lax.broadcasted_iota(jnp.int32, req_out.shape[1:], 0)
    for c in range(PLANE):
        tile = jnp.zeros(req_out.shape[1:], jnp.int32)
        for z in range(depth):
            tile = jnp.where(row_at == z, local_of[z * PLANE + c], tile)
        req_out[c] = tile

    for load in loads[3:]:
        load.start()

    def peer(i):
        step = lax.div(i, PLANE)
        dz = jnp.where(my_z * 2 < depth, step, lax.rem(depth - step, depth))
        return lax.rem(my_z + dz, depth), lax.rem(my_q + lax.rem(i, PLANE), PLANE)

    def exchange(out_ref, in_ref, send, recv, i):
        z, c = peer(i)
        target = z * PLANE + c
        return pltpu.make_async_remote_copy(
            src_ref=out_ref.at[target],
            dst_ref=in_ref.at[me],
            send_sem=send,
            recv_sem=recv,
            device_id={"st": target},
            device_id_type=MESH,
        )

    def bulk(ref, send, recv):
        return pltpu.make_async_remote_copy(
            src_ref=ref,
            dst_ref=ref,
            send_sem=send,
            recv_sem=recv,
            device_id={"tp": 1 - tp},
            device_id_type=MESH,
        )

    def bulk_all(out_ref, in_ref, send, recv):
        return bulk(in_ref.at[pl.ds(0, n - 1)], send, recv)

    def start_some(lo, hi, *refs):
        def body(i, carry):
            exchange(*refs, i).start()
            return carry

        lax.fori_loop(lo, hi, body, 0)

    def ask(i, far):
        z, c = peer(i)
        return pltpu.make_async_remote_copy(
            src_ref=req_out.at[c],
            dst_ref=req_in.at[me],
            send_sem=req_send.at[far],
            recv_sem=req_recv.at[far],
            device_id={"st": z * PLANE + c},
            device_id_type=MESH,
        )

    asked_near = bulk(req_in.at[pl.ds(0, PLANE - 1)], req_send.at[0], req_recv.at[0])
    asked_far = bulk(req_in.at[pl.ds(0, n - PLANE)], req_send.at[1], req_recv.at[1])
    gks = [
        (gk_out.at[c], gk_in.at[c], gk_send.at[c], gk_recv.at[c]) for c in range(PARTS)
    ]

    pl.semaphore_wait(
        barrier, PLANE + has_up.astype(jnp.int32) + has_down.astype(jnp.int32)
    )
    for i in range(1, PLANE):
        ask(i, 0).start()
    req_in[me] = req_out[my_q]

    grain = plen // CHUNKS

    def grain_of(p):
        return pl.ds(pl.multiple_of(p * grain, grain), grain)

    def along(up, z, p):
        at = kv_col.at[z, :, grain_of(p)]
        return pltpu.make_async_remote_copy(
            src_ref=at,
            dst_ref=at,
            send_sem=z_send.at[up, z],
            recv_sem=z_recv.at[z, p],
            device_id={"st": me + (2 * up - 1) * PLANE},
            device_id_type=MESH,
        )

    for load in loads[:3]:
        load.wait()
    own_shape = (pass_dev, plen, HEAD)
    kv_col[my_z, :, :, :HEAD] = nn(store[...], wk[...]).astype(BF).reshape(own_shape)
    kv_col[my_z, :, :, HEAD:] = nn(store[...], wv[...]).astype(BF).reshape(own_shape)
    for p in range(CHUNKS):

        @pl.when(has_up)
        def _():
            along(1, my_z, p).start()

        @pl.when(has_down)
        def _():
            along(0, my_z, p).start()

    def names(row, p, lanes):
        mask = jnp.where(row == p, 1.0, 0.0).astype(F32)
        return jnp.concatenate([mask] * (lanes // mask.shape[1]), axis=1)

    def hand(z, p, i):
        return pltpu.make_async_remote_copy(
            src_ref=kv_out.at[z, i - 1, grain_of(p)],
            dst_ref=kv_in.at[z * PLANE + my_q, grain_of(p)],
            send_sem=kv_send.at[0],
            recv_sem=kv_recv.at[0],
            device_id={"st": my_z * PLANE + lax.rem(my_q + i, PLANE)},
            device_id_type=MESH,
        )

    def spread(z, p):
        rows = [kv_col[z, k, grain_of(p), :].astype(F32) for k in range(pass_dev)]

        def pick(reader):
            row = req_in[my_z * PLANE + reader, pl.ds(z, 1), :]
            chosen = names(row, 0, 2 * HEAD) * rows[0]
            for k in range(1, pass_dev):
                chosen = chosen + names(row, k, 2 * HEAD) * rows[k]
            return chosen.astype(BF)

        for i in range(1, PLANE):
            kv_out[z, i - 1, grain_of(p), :] = pick(lax.rem(my_q + i, PLANE))
        kv_in[z * PLANE + my_q, grain_of(p), :] = pick(my_q)
        for i in range(1, PLANE):
            hand(z, p, i).start()

    def pump(k, p):
        def side(up, carry):
            z = my_z + k * (1 - 2 * up)

            @pl.when((z >= 0) & (z < depth))
            def _():
                along(up, z, p).wait_recv()

                @pl.when(jnp.where(up == 1, has_up, has_down))
                def _():
                    along(up, z, p).start()

                spread(z, p)

            return carry

        lax.fori_loop(0, 2, side, 0)

    quarter = width // PLANE
    share = quarter // 2

    def share_rows(i):
        other = lax.rem(my_q + i, PLANE)
        return pltpu.make_async_remote_copy(
            src_ref=store.at[:, pl.ds(pl.multiple_of(other * quarter + tp * share, share), share)],
            dst_ref=slices.at[tp, i - 1],
            send_sem=rows_send.at[0],
            recv_sem=rows_recv.at[0],
            device_id={"st": my_z * PLANE + other},
            device_id_type=MESH,
        )

    rows_shared = bulk(slices.at[tp], rows_send.at[0], rows_recv.at[0])
    rows_swap = bulk(slices.at[tp], swap_send.at[0], swap_recv.at[0])
    rows_swapped = bulk(slices.at[1 - tp], swap_send.at[0], swap_recv.at[0])

    def project(w, out, then=None):
        def body(i, carry):
            cols = pl.ds(pl.multiple_of(i * TILE, TILE), TILE)
            out[:, cols] = nn(tokens[...], w[:, cols]).astype(BF)
            if then is not None:
                then(i)
            return carry

        lax.fori_loop(0, w.shape[1] // TILE, body, 0)

    loads[3].wait()
    for load, w, out in ((loads[4], wrq, rq), (loads[5], wrk, rk)):
        load.wait()
        project(w, out)
    asked_near.wait_recv()

    def spread_own(p, carry):
        spread(my_z, p)
        return carry

    lax.fori_loop(0, CHUNKS, spread_own, 0)
    for i in range(1, PLANE):
        share_rows(i).start()
    loads[6].wait()
    project(wrv, rv)
    loads[7].wait()

    ret_key = rq.shape[1] // ret_heads
    ret_value = rv.shape[1] // ret_heads
    at_t = lax.broadcasted_iota(jnp.int32, (length, length), 0)
    at_s = lax.broadcasted_iota(jnp.int32, (length, length), 1)
    distance = (at_t - at_s).astype(F32)

    def retention(j, carry):
        kc = pl.ds(pl.multiple_of(j * ret_key, ret_key), ret_key)
        vc = pl.ds(pl.multiple_of(j * ret_value, ret_value), ret_value)
        damping = jnp.where(
            distance >= 0.0, jnp.exp(-rate_ref[j] * jnp.maximum(distance, 0.0)), 0.0
        ) * ret_key ** (-0.5)
        weights = (nt(rq[:, kc], rk[:, kc]) * damping).astype(BF)
        y = nn(weights, rv[:, vc])
        r = lax.rsqrt(jnp.mean(y * y, axis=1, keepdims=True) + EPSILON)
        c = og[:, vc].astype(F32) * gain_ref[:, vc]
        inner = jnp.mean(c * y, axis=1, keepdims=True)
        gy = (r * c - r * r * r * y * inner).astype(BF)
        gw = (nt(gy, rv[:, vc]) * damping).astype(BF)
        grq[:, kc] = nn(gw, rk[:, kc]).astype(BF)
        grk[:, kc] = tn(gw, rq[:, kc]).astype(BF)
        grv[:, vc] = tn(weights, gy).astype(BF)
        pump(1, j)
        return carry

    lax.fori_loop(0, ret_heads, retention, 0)
    loads[8].wait()
    project(wq, q, lambda i: pump(2, i))

    def ret_total(i, carry):
        wide = width // CHUNKS
        rows = pl.ds(pl.multiple_of(i * wide, wide), wide)
        total[:, rows] = (
            nt(grq[...], wrq[rows, :]) + nt(grk[...], wrk[rows, :]) + nt(grv[...], wrv[rows, :])
        )
        pump(3, i)
        return carry

    lax.fori_loop(0, CHUNKS, ret_total, 0)
    rows_shared.wait_recv()
    rows_swap.start()
    cols = [slice(g * HEAD, (g + 1) * HEAD) for g in range(group)]
    gate = 1.0 / (1.0 + jnp.exp(-gate_ref[...]))

    def gated(b, carry):
        rows = pl.ds(pl.multiple_of(b * BLK, BLK), BLK)
        for g, c in enumerate(cols):
            at = slice(g * BLK, (g + 1) * BLK)
            grad_attn = og[rows, c].astype(F32) * gate[:, c]
            ga[b, at, :] = grad_attn
            ga_bf[b, at, :] = grad_attn.astype(BF)
        return carry

    lax.fori_loop(0, blocks, gated, 0)
    bulk(kv_in.at[pl.ds(0, n - depth)], kv_send.at[0], kv_recv.at[0]).wait_recv()

    def ask_far(i, carry):
        ask(i, 1).start()
        return carry

    lax.fori_loop(PLANE, n, ask_far, 0)
    factor = HEAD ** (-0.5)

    def attend(step, carry):
        group_of = [step * TOGETHER + t for t in range(TOGETHER)]
        rows = [pl.ds(pl.multiple_of(b * BLK, BLK), BLK) for b in group_of]
        read = [[kv_in[owner_of[b * KP + k]] for k in range(KP)] for b in group_of]
        keys = [jnp.concatenate([x[:, :HEAD] for x in each], axis=0) for each in read]
        values = [jnp.concatenate([x[:, HEAD:] for x in each], axis=0) for each in read]
        queries = [jnp.concatenate([q[r, c] for c in cols], axis=0) for r in rows]
        expo = [jnp.exp(nt(a, b) * factor) for a, b in zip(queries, keys)]
        grad_probs = [nt(ga_bf[b], v) for b, v in zip(group_of, values)]
        probs = [e / jnp.sum(e, axis=1, keepdims=True) for e in expo]
        probs_bf = [x.astype(BF) for x in probs]
        attn = [nn(x, v) for x, v in zip(probs_bf, values)]
        delta = [
            jnp.sum(ga[b] * a, axis=1, keepdims=True) for b, a in zip(group_of, attn)
        ]
        scores = [
            (x * (g - d) * factor).astype(BF) for x, g, d in zip(probs, grad_probs, delta)
        ]
        dk = [tn(x, a).astype(BF) for x, a in zip(scores, queries)]
        dv = [tn(x, ga_bf[b]).astype(BF) for x, b in zip(probs_bf, group_of)]
        grad_query = [nn(x, a).astype(BF) for x, a in zip(scores, keys)]
        for t, b in enumerate(group_of):
            for g, c in enumerate(cols):
                gq[rows[t], c] = grad_query[t][g * BLK : (g + 1) * BLK, :]
            for k in range(KP):
                at = slice(k * plen, (k + 1) * plen)
                for c in range(PARTS):
                    stage_k[c, b * KP + k] = dk[t][at, c * SPAN : (c + 1) * SPAN]
                stage_v[b * KP + k] = dv[t][at, :]
        return carry

    lax.fori_loop(0, blocks // TOGETHER, attend, 0)

    def place(stage, out):
        def body(o, carry):
            out[o] = stage[slot_of[o]]
            return carry

        lax.fori_loop(0, n, body, 0)

    is_end = (my_z == 0) | (my_z == depth - 1)
    upper = my_z * 2 >= depth
    near_end = jnp.where(upper, depth - 1, 0)
    near_mid = jnp.where(upper, depth - 2, 1)
    far_end = depth - 1 - near_end
    far_mid = depth - 1 - near_mid

    def hand_value(z, i, part):
        mate = lax.rem(my_q + i, PLANE)
        return pltpu.make_async_remote_copy(
            src_ref=gv_out.at[z * PLANE + mate],
            dst_ref=v_in.at[z, my_q],
            send_sem=v_send.at[part],
            recv_sem=v_recv.at[part],
            device_id={"st": my_z * PLANE + mate},
            device_id_type=MESH,
        )

    place(stage_k.at[0], gk_out.at[0])
    start_some(1, n, *gks[0])
    place(stage_k.at[1], gk_out.at[1])
    place(stage_v, gv_out)
    for c in range(PARTS):
        gk_in[c, me] = gk_out[c, me]
    for z in range(depth):
        v_in[z, my_q] = gv_out[z * PLANE + my_q]

    def finish_total(i, carry):
        rows = pl.ds(pl.multiple_of(i * TILE, TILE), TILE)
        gt[:, rows] = (total[:, rows] + nt(gq[...], wq[rows, :])).astype(BF)
        return carry

    lax.fori_loop(0, width // TILE, finish_total, 0)
    for z in (far_end, far_mid):
        for i in range(1, PLANE):
            hand_value(z, i, 0).start()

    def to_partner(out_ref, in_ref, half, at):
        return pltpu.make_async_remote_copy(
            src_ref=out_ref.at[pl.ds(pl.multiple_of((1 - tp) * half, half), half)],
            dst_ref=in_ref,
            send_sem=tp_send.at[at],
            recv_sem=tp_recv.at[at],
            device_id={"tp": 1 - tp},
            device_id_type=MESH,
        )

    def add_own(out_ref, in_ref, half):
        own = out_ref[pl.ds(pl.multiple_of(tp * half, half), half), :]
        in_ref[...] = (own.astype(F32) + in_ref[...].astype(F32)).astype(BF)

    token_swap = to_partner(gt, gt_in, half_tok, 0)
    token_swap.start()

    def gather_sum(in_ref, out_ref):
        lanes = out_ref.shape[1]

        def body(r, sums):
            row = req_in[r, pl.ds(my_z, 1), :]
            term = in_ref[r].astype(F32)
            return tuple(s + names(row, p, lanes) * term for p, s in enumerate(sums))

        sums = lax.fori_loop(0, n, body, (jnp.zeros((plen, lanes), F32),) * pass_dev)
        for p, s in enumerate(sums):
            out_ref[p * plen : (p + 1) * plen, :] = s.astype(BF)

    def share_key(c, i):
        return pltpu.make_async_remote_copy(
            src_ref=pk.at[c],
            dst_ref=pk_in.at[c, i - 1],
            send_sem=pk_send.at[c],
            recv_sem=pk_recv.at[c],
            device_id={"st": my_z * PLANE + lax.rem(my_q + i, PLANE)},
            device_id_type=MESH,
        )

    def column_reduce(c, i):
        other = lax.rem(my_z + i, depth)
        return pltpu.make_async_remote_copy(
            src_ref=p1_sum.at[c, other],
            dst_ref=p2_in.at[c, i - 1],
            send_sem=p2_send.at[c],
            recv_sem=p2_recv.at[c],
            device_id={"st": other * PLANE + my_q},
            device_id_type=MESH,
        )

    def column_gather(c, up, z):
        at = kg.at[c, my_q * depth + z]
        return pltpu.make_async_remote_copy(
            src_ref=at,
            dst_ref=at,
            send_sem=p3_send.at[up, c],
            recv_sem=p3_recv.at[c, z],
            device_id={"st": me + (2 * up - 1) * PLANE},
            device_id_type=MESH,
        )

    def plane_gather(c, i, z):
        at = kg.at[c, my_q * depth + z]
        return pltpu.make_async_remote_copy(
            src_ref=at,
            dst_ref=at,
            send_sem=p4_send.at[c],
            recv_sem=p4_recv.at[c],
            device_id={"st": my_z * PLANE + lax.rem(my_q + i, PLANE)},
            device_id_type=MESH,
        )

    def send_part(at, dst, sem, z):
        return pltpu.make_async_remote_copy(
            src_ref=vp_out.at[at],
            dst_ref=dst,
            send_sem=vp_send.at[0],
            recv_sem=vp_recv.at[sem],
            device_id={"st": z * PLANE + my_q},
            device_id_type=MESH,
        )

    def merge(z, out_ref, *more):
        def body(p, carry):
            at = pl.ds(pl.multiple_of(p * plen, plen), plen)
            acc = jnp.zeros((plen, HEAD), F32)
            for r in range(PLANE):
                row = req_in[my_z * PLANE + r, pl.ds(z, 1), :]
                acc = acc + names(row, p, HEAD) * v_in[z, r].astype(F32)
            for ref in more:
                acc = acc + ref[at, :].astype(F32)
            out_ref[at, :] = acc.astype(BF)
            return carry

        lax.fori_loop(0, pass_dev, body, 0)

    def pass_near():
        z = jnp.where(is_end, near_mid, near_end)
        merge(z, vp_out.at[2])
        send_part(2, v_add.at[0], 2, z).start()

    def pass_first(which):
        z = (far_mid, far_end)[which]

        @pl.when(is_end)
        def _():
            merge(z, vp_out.at[which])
            send_part(which, v_mid.at[which], which, near_mid).start()

    def pass_second(which):
        z = (far_mid, far_end)[which]

        @pl.when(jnp.logical_not(is_end))
        def _():
            bulk(v_mid.at[which], vp_send.at[0], vp_recv.at[which]).wait_recv()
            merge(z, vp_out.at[which], v_mid.at[which])
            send_part(which, v_add.at[1], 3, z).start()

    rows_swapped.wait_recv()
    asked_far.wait_recv()

    own_cols = pl.ds(pl.multiple_of(my_q * quarter, quarter), quarter)
    own_terms = []
    for c in range(PARTS):
        bulk_all(*gks[c]).wait_recv()
        if c == 0:
            start_some(1, n, *gks[1])
        gather_sum(gk_in.at[c], pk.at[c])
        for i in range(1, PLANE):
            share_key(c, i).start()
        own_terms.append(tn(store[:, own_cols], pk[c]))
        if c == 0:
            for z in (near_mid, near_end):
                for i in range(1, PLANE):
                    hand_value(z, i, 1).start()
    v_half = [bulk(gv_out.at[pl.ds(0, 2 * (PLANE - 1))], v_send.at[h], v_recv.at[h]) for h in range(2)]

    token_swap.wait_recv()
    add_own(gt, gt_in, half_tok)
    token_out = pltpu.make_async_copy(gt_in, gt_hbm, out_sem.at[0])
    token_out.start()

    for c in range(PARTS):
        bulk(pk_in.at[c], pk_send.at[c], pk_recv.at[c]).wait_recv()
        for part in range(2):
            acc = own_terms[c][part * share : (part + 1) * share]
            for i in range(1, PLANE):
                acc = acc + tn(slices[part, i - 1], pk_in[c, i - 1])
            acc = acc.reshape(depth // 2, -1, SPAN)
            p1_sum[c, part * depth // 2 : (part + 1) * depth // 2] = acc.astype(BF)
        for i in range(1, depth):
            column_reduce(c, i).start()
        if c == 0:
            v_half[0].wait_recv()
            pass_first(0)

    def key_store_grad(i, carry):
        rows = pl.ds(pl.multiple_of(i * TILE, TILE), TILE)
        keys = jnp.concatenate([pk[c] for c in range(PARTS)], axis=1)
        gs_key[:, rows] = nt(keys, wk[rows, :])
        return carry

    lax.fori_loop(0, width // TILE, key_store_grad, 0)

    for c in range(PARTS):
        bulk(p2_in.at[c], p2_send.at[c], p2_recv.at[c]).wait_recv()
        acc = p1_sum[c, my_z].astype(F32)
        for i in range(1, depth):
            acc = acc + p2_in[c, i - 1].astype(F32)
        kg[c, my_q * depth + my_z] = acc.astype(BF)

        @pl.when(has_up)
        def _():
            column_gather(c, 1, my_z).start()

        @pl.when(has_down)
        def _():
            column_gather(c, 0, my_z).start()

        for i in range(1, PLANE):
            plane_gather(c, i, my_z).start()
        if c == 0:
            pass_first(1)
            pass_second(0)

    v_half[1].wait_recv()
    pass_near()

    def relay(step, carry):
        k = 1 + lax.div(step, 2 * PARTS)
        c = lax.rem(lax.div(step, 2), PARTS)
        up = lax.rem(step, 2)
        z = my_z + k * (1 - 2 * up)

        @pl.when((z >= 0) & (z < depth))
        def _():
            column_gather(c, up, z).wait_recv()

            @pl.when(jnp.where(up == 1, has_up, has_down))
            def _():
                column_gather(c, up, z).start()

            for i in range(1, PLANE):
                plane_gather(c, i, z).start()

        return carry

    lax.fori_loop(0, 2 * PARTS, relay, 0)
    pass_second(1)
    lax.fori_loop(2 * PARTS, 2 * PARTS * (depth - 1), relay, 0)

    for sem in range(2):
        bulk(v_add.at[sem], vp_send.at[0], vp_recv.at[2 + sem]).wait_recv()
    merge(my_z, pv, v_add.at[0], v_add.at[1])
    wide = width // SWAPS

    def cut(i):
        return pl.ds(pl.multiple_of(i * wide, wide), wide)

    def half_of(which):
        return pl.ds(pl.multiple_of(which * half_store, half_store), half_store)

    def store_swap(i):
        return pltpu.make_async_remote_copy(
            src_ref=gs.at[half_of(1 - tp), cut(i)],
            dst_ref=gs_in.at[:, cut(i)],
            send_sem=tp_send.at[1 + i],
            recv_sem=tp_recv.at[1 + i],
            device_id={"tp": 1 - tp},
            device_id_type=MESH,
        )

    def store_grad(i, carry):
        gs[:, cut(i)] = (gs_key[:, cut(i)] + nt(pv[...], wv[cut(i), :])).astype(BF)
        store_swap(i).start()
        return carry

    lax.fori_loop(0, SWAPS, store_grad, 0)

    def store_sum(i, carry):
        store_swap(i).wait_recv()
        own = gs[half_of(tp), cut(i)]
        gs_in[:, cut(i)] = (own.astype(F32) + gs_in[:, cut(i)].astype(F32)).astype(BF)
        return carry

    lax.fori_loop(0, SWAPS, store_sum, 0)
    store_out = pltpu.make_async_copy(gs_in, gs_hbm, out_sem.at[1])
    store_out.start()

    weight_out = []
    for c in range(PARTS):
        bulk(kg.at[c, pl.ds(0, n - depth)], p4_send.at[c], p4_recv.at[c]).wait_recv()
        weight_out.append(pltpu.make_async_copy(kg.at[c], gkw_hbm.at[c], out_sem.at[2 + c]))
        weight_out[c].start()

    asked_near.wait_send()
    asked_far.wait_send()
    for z in range(depth):

        @pl.when(has_up & (z <= my_z))
        def _():
            bulk(kv_col.at[z], z_send.at[1, z], z_recv.at[z, 0]).wait_send()

        @pl.when(has_down & (z >= my_z))
        def _():
            bulk(kv_col.at[z], z_send.at[0, z], z_recv.at[z, 0]).wait_send()

    bulk(kv_out, kv_send.at[0], kv_recv.at[0]).wait_send()
    for half in v_half:
        half.wait_send()
    bulk(vp_out, vp_send.at[0], vp_recv.at[0]).wait_send()
    token_swap.wait_send()
    for i in range(SWAPS):
        store_swap(i).wait_send()
    for c in range(PARTS):
        bulk_all(*gks[c]).wait_send()
        bulk(pk_in.at[c], pk_send.at[c], pk_recv.at[c]).wait_send()
        bulk(kg.at[c, pl.ds(0, n - depth)], p4_send.at[c], p4_recv.at[c]).wait_send()
        bulk(p2_in.at[c], p2_send.at[c], p2_recv.at[c]).wait_send()
    for z in range(depth):

        @pl.when(my_z == z)
        def _():
            for c in range(PARTS):
                if z < depth - 1:
                    at = kg.at[c, pl.ds(0, z + 1)]
                    bulk(at, p3_send.at[1, c], p3_recv.at[c, 0]).wait_send()
                if z > 0:
                    at = kg.at[c, pl.ds(0, depth - z)]
                    bulk(at, p3_send.at[0, c], p3_recv.at[c, 0]).wait_send()

    rows_shared.wait_send()
    rows_swap.wait_send()
    token_out.wait()
    store_out.wait()
    for out in weight_out:
        out.wait()


def finish_kernel(gt_hbm, gs_hbm, kg_hbm, ot_hbm, os_hbm, ok_hbm, gt, gs, kg, out, in_sem, out_sem):
    pieces = in_sem.shape[0] - 2
    span = out.shape[0] // pieces
    cuts = [pl.ds(i * span, span) for i in range(pieces)]
    loads = [
        pltpu.make_async_copy(kg_hbm.at[:, at], kg.at[:, at], in_sem.at[i])
        for i, at in enumerate(cuts)
    ]
    loads += [
        pltpu.make_async_copy(gt_hbm, gt, in_sem.at[pieces]),
        pltpu.make_async_copy(gs_hbm, gs, in_sem.at[pieces + 1]),
    ]
    for load in loads:
        load.start()
    stores = []
    for i, at in enumerate(cuts):
        loads[i].wait()
        for c in range(PARTS):
            out[at, c * SPAN : (c + 1) * SPAN] = kg[c, at, :].astype(F32)
        stores.append(pltpu.make_async_copy(out.at[at], ok_hbm.at[at], out_sem.at[i]))
        stores[-1].start()
    for i, (a, b) in enumerate(((gt, ot_hbm), (gs, os_hbm))):
        loads[pieces + i].wait()
        stores.append(pltpu.make_async_copy(a, b, out_sem.at[pieces + i]))
        stores[-1].start()
    for store in stores:
        store.wait()


def per_device(sizes, *args):
    (tokens, store, ids, wq, wk, wv, wrq, wrk, wrv, rate, gain, gate, og) = args
    n = sizes["st"]
    pass_dev, plen, width = store.shape
    length = tokens.shape[0]
    rows = pass_dev * plen
    weight_cols = sum(w.shape[1] for w in (wq, wk, wv, wrq, wrk, wrv))
    fits = (
        sizes["tp"] == 2
        and wk.shape[1] == HEAD
        and HEAD == PARTS * SPAN
        and ids.size == n
        and n == PLANE * 4
        and plen % (16 * CHUNKS) == 0
        and length % (BLK * TOGETHER) == 0
        and rate.shape[0] == CHUNKS
        and wq.shape[1] == CHUNKS * TILE
        and width % (n * 128) == 0
        and width * weight_cols + n * plen * HEAD * 12 + length * width * 12 < 24 * 2**20
    )
    if not fits:
        return per_device_plain(*args)
    depth = n // PLANE
    piece = width // n

    def vm(*shape, dtype=BF):
        return pltpu.VMEM(shape, dtype)

    any_spec = pl.BlockSpec(memory_space=pl.ANY)
    smem = pl.BlockSpec(memory_space=pltpu.SMEM)
    vmem = pl.BlockSpec(memory_space=pltpu.VMEM)
    dma = pltpu.SemaphoreType.DMA
    like = [vm(*x.shape) for x in (tokens,)] + [vm(rows, width)]
    like += [vm(*x.shape) for x in (wq, wk, wv, wrq, wrk, wrv, og)]
    qs = [vm(length, w.shape[1]) for w in (wq, wrq, wrk, wrv)]
    scratch = (
        like
        + qs
        + qs
        + [
            vm(length, width, dtype=F32),
            vm(length, width),
            vm(length // 2, width),
            vm(rows, width, dtype=F32),
            vm(rows, width),
            vm(rows // 2, width),
            vm(length // BLK, BLK * wq.shape[1] // HEAD, HEAD, dtype=F32),
            vm(length // BLK, BLK * wq.shape[1] // HEAD, HEAD),
            vm(depth, pass_dev, plen, 2 * HEAD),
            vm(depth, PLANE - 1, plen, 2 * HEAD),
            vm(n, plen, 2 * HEAD),
            vm(PLANE, 8, 128, dtype=jnp.int32),
            vm(n, 8, 128, dtype=jnp.int32),
            vm(PARTS, n, plen, SPAN),
            vm(n, plen, HEAD),
            vm(PARTS, n, plen, SPAN),
            vm(n, plen, HEAD),
            vm(PARTS, n, plen, SPAN),
            vm(depth, PLANE, plen, HEAD),
            vm(3, rows, HEAD),
            vm(2, rows, HEAD),
            vm(2, rows, HEAD),
            vm(PARTS, rows, SPAN),
            vm(rows, HEAD),
            vm(2, PLANE - 1, rows, width // (2 * PLANE)),
            vm(PARTS, PLANE - 1, rows, SPAN),
            vm(PARTS, depth, piece, SPAN),
            vm(PARTS, depth - 1, piece, SPAN),
            vm(PARTS, n, piece, SPAN),
            pltpu.SMEM((n,), jnp.int32),
            pltpu.SMEM((n,), jnp.int32),
            pltpu.SMEM((n,), jnp.int32),
            dma((9,)),
            dma((2 + PARTS,)),
        ]
        + [dma((1 + SWAPS,))] * 2
        + [dma((2,))] * 2
        + [dma((2,))] * 2
        + [dma((1,)), dma((4,))]
        + [dma((PARTS,))] * 2
        + [dma((2, depth)), dma((depth, CHUNKS))]
        + [dma((1,))] * 6
        + [dma((PARTS,))] * 4
        + [dma((2, PARTS)), dma((PARTS, depth))]
        + [dma((PARTS,))] * 2
    )
    grad_tokens, grad_store, grad_key = pl.pallas_call(
        functools.partial(fused_kernel, n),
        out_shape=(
            jax.ShapeDtypeStruct((length // 2, width), BF),
            jax.ShapeDtypeStruct((rows // 2, width), BF),
            jax.ShapeDtypeStruct((PARTS, n, piece, SPAN), BF),
        ),
        in_specs=[smem, smem, vmem, vmem] + [any_spec] * 9,
        out_specs=(any_spec, any_spec, any_spec),
        scratch_shapes=scratch,
        compiler_params=pltpu.CompilerParams(
            collective_id=0, has_side_effects=True, vmem_limit_bytes=60 * 2**20
        ),
    )(
        ids,
        rate,
        gain.reshape(1, -1),
        gate.reshape(1, -1),
        tokens,
        store.reshape(rows, width),
        wq,
        wk,
        wv,
        wrq,
        wrk,
        wrv,
        og,
    )
    grad_tokens, grad_store, grad_key = pl.pallas_call(
        finish_kernel,
        out_shape=(
            jax.ShapeDtypeStruct((length // 2, width), BF),
            jax.ShapeDtypeStruct((rows // 2, width), BF),
            jax.ShapeDtypeStruct((width, HEAD), F32),
        ),
        in_specs=[any_spec] * 3,
        out_specs=(any_spec, any_spec, any_spec),
        scratch_shapes=[
            vm(length // 2, width),
            vm(rows // 2, width),
            vm(PARTS, width, SPAN),
            vm(width, HEAD, dtype=F32),
            dma((6,)),
            dma((6,)),
        ],
    )(grad_tokens, grad_store, grad_key.reshape(PARTS, width, SPAN))
    return (grad_tokens, grad_store.reshape(pass_dev // 2, plen, width), grad_key)


def solution(mesh):
    return jax.shard_map(
        functools.partial(per_device, dict(mesh.shape)),
        mesh=mesh,
        in_specs=(
            P("st", None),
            P("st", None, None),
            P("st", None),
            P(None, "tp"),
            P(None, "tp"),
            P(None, "tp"),
            P(None, "tp"),
            P(None, "tp"),
            P(None, "tp"),
            P("tp"),
            P("tp"),
            P("tp"),
            P("st", "tp"),
        ),
        out_specs=(P(("st", "tp"), None), P(("st", "tp"), None, None), P(None, "tp")),
        check_vma=False,
    )
```

```python
import functools

import jax
import jax.numpy as jnp
from jax import lax
from jax.experimental import pallas as pl
from jax.experimental.pallas import tpu as pltpu
from jax.sharding import PartitionSpec as P

HEAD = 256
BLK = 64
KP = 4
MOST = 1


EPSILON = 1.0


def retention_grads(query_rows, key_rows, value_rows, rates, gains, cotangent):
    length = query_rows.shape[0]
    heads = rates.shape[0]
    queries = query_rows.reshape(length, heads, -1)
    keyset = key_rows.reshape(length, heads, -1)
    values = value_rows.reshape(length, heads, -1)
    positions = jnp.arange(length, dtype=jnp.float32)
    distance = positions[:, None] - positions[None, :]
    damping = jnp.where(
        distance >= 0.0, jnp.exp(-rates[:, None, None] * jnp.maximum(distance, 0.0)), 0.0
    ) * queries.shape[-1] ** (-0.5)
    raw = jnp.einsum("thd,shd->hts", queries, keyset, preferred_element_type=jnp.float32)
    weights = (raw * damping).astype(jnp.bfloat16)
    mixed = jnp.einsum("hts,she->the", weights, values, preferred_element_type=jnp.float32)
    inverse = lax.rsqrt(jnp.mean(mixed * mixed, axis=-1, keepdims=True) + EPSILON)
    scaled = cotangent.astype(jnp.float32).reshape(length, heads, -1) * gains.reshape(heads, -1)
    inner = jnp.mean(scaled * mixed, axis=-1, keepdims=True)
    grad_mixed = (inverse * scaled - inverse * inverse * inverse * mixed * inner).astype(
        jnp.bfloat16
    )
    grad_weights = (
        jnp.einsum("the,she->hts", grad_mixed, values, preferred_element_type=jnp.float32) * damping
    ).astype(jnp.bfloat16)
    grad_first = (
        jnp.einsum("hts,shd->thd", grad_weights, keyset, preferred_element_type=jnp.float32)
        .astype(jnp.bfloat16)
        .reshape(length, -1)
    )
    grad_second = (
        jnp.einsum("hts,thd->shd", grad_weights, queries, preferred_element_type=jnp.float32)
        .astype(jnp.bfloat16)
        .reshape(length, -1)
    )
    grad_third = (
        jnp.einsum("hts,the->she", weights, grad_mixed, preferred_element_type=jnp.float32)
        .astype(jnp.bfloat16)
        .reshape(length, -1)
    )
    return (grad_first, grad_second, grad_third)


def against_rows(left, weight):
    return lax.dot_general(
        left, weight, (((1,), (1,)), ((), ())), preferred_element_type=jnp.float32
    )


def across_rows(left, right):
    return lax.dot_general(
        left, right, (((0,), (0,)), ((), ())), preferred_element_type=jnp.float32
    )


def per_device_plain(
    tokens,
    store,
    passage_ids,
    w_query,
    w_key,
    w_value,
    w_ret_query,
    w_ret_key,
    w_ret_value,
    ret_rate,
    ret_gain,
    gate_logit,
    out_grad,
):
    owners = lax.axis_size("st")
    pass_dev, plen, width = store.shape
    length = tokens.shape[0]
    kv_width = w_key.shape[1]
    kv_local = kv_width // HEAD
    group = w_query.shape[1] // HEAD // kv_local
    blocks = length // BLK
    slot_ids = passage_ids.reshape(-1)
    slot_count = slot_ids.shape[0]
    slot_owner = slot_ids // pass_dev
    slot_local = slot_ids % pass_dev
    order = jnp.arange(slot_count, dtype=jnp.int32)
    same_owner = slot_owner[:, None] == slot_owner[None, :]
    rank = jnp.sum(same_owner & (order[None, :] < order[:, None]), axis=1)
    position = slot_owner * MOST + rank
    cells = owners * MOST
    placed = jnp.arange(cells, dtype=jnp.int32)[:, None] == position[None, :]
    request = (jnp.sum(jnp.where(placed, slot_local[None, :] + 1, 0), axis=1) - 1).reshape(
        owners, MOST
    )
    incoming = lax.all_to_all(request, "st", split_axis=0, concat_axis=0, tiled=True)
    wanted = incoming.reshape(-1)
    valid = wanted >= 0
    safe = jnp.maximum(wanted, 0)
    placed_bf = placed.astype(jnp.bfloat16)
    store_rows = store.reshape(-1, width)
    nothing = jnp.zeros((), jnp.bfloat16)
    own_kv = jnp.concatenate(
        [
            jnp.dot(store_rows, w_key, preferred_element_type=jnp.float32).astype(jnp.bfloat16),
            jnp.dot(store_rows, w_value, preferred_element_type=jnp.float32).astype(jnp.bfloat16),
        ],
        axis=1,
    ).reshape(pass_dev, plen, 2 * kv_width)
    reply = jnp.where(valid[:, None, None], own_kv[safe], nothing).reshape(
        owners, MOST, plen, 2 * kv_width
    )
    arrived = lax.all_to_all(reply, "st", split_axis=0, concat_axis=0, tiled=True)
    slot_kv = (
        across_rows(placed_bf, arrived.reshape(cells, -1))
        .astype(jnp.bfloat16)
        .reshape(slot_count, plen, 2 * kv_width)
    )
    factor = HEAD ** (-0.5)
    gate = jax.nn.sigmoid(gate_logit)
    query_bf = jnp.dot(tokens, w_query, preferred_element_type=jnp.float32).astype(jnp.bfloat16)
    queries = query_bf.reshape(blocks, BLK, kv_local, group, HEAD)
    keys = slot_kv[:, :, :kv_width].reshape(blocks, KP * plen, kv_local, HEAD)
    values = slot_kv[:, :, kv_width:].reshape(blocks, KP * plen, kv_local, HEAD)
    scores = (
        jnp.einsum("btkgd,bskd->bkgts", queries, keys, preferred_element_type=jnp.float32) * factor
    )
    expo = jnp.exp(scores)
    probs = expo / jnp.sum(expo, axis=-1, keepdims=True)
    probs_bf = probs.astype(jnp.bfloat16)
    attn = jnp.einsum("bkgts,bskd->btkgd", probs_bf, values, preferred_element_type=jnp.float32)
    grad_attn = out_grad.astype(jnp.float32).reshape(
        blocks, BLK, kv_local, group, HEAD
    ) * gate.reshape(kv_local, group, HEAD)
    grad_attn_bf = grad_attn.astype(jnp.bfloat16)
    grad_probs = jnp.einsum(
        "btkgd,bskd->bkgts", grad_attn_bf, values, preferred_element_type=jnp.float32
    )
    delta = jnp.moveaxis(jnp.sum(grad_attn * attn, axis=-1), 1, 3)
    grad_scores = (probs * (grad_probs - delta[..., None]) * factor).astype(jnp.bfloat16)
    grad_query = (
        jnp.einsum("bkgts,bskd->btkgd", grad_scores, keys, preferred_element_type=jnp.float32)
        .astype(jnp.bfloat16)
        .reshape(length, -1)
    )
    grad_keys = (
        jnp.einsum("bkgts,btkgd->bskd", grad_scores, queries, preferred_element_type=jnp.float32)
        .astype(jnp.bfloat16)
        .reshape(slot_count, plen, kv_width)
    )
    grad_values = (
        jnp.einsum("bkgts,btkgd->bskd", probs_bf, grad_attn_bf, preferred_element_type=jnp.float32)
        .astype(jnp.bfloat16)
        .reshape(slot_count, plen, kv_width)
    )
    slot_grad = jnp.concatenate([grad_keys, grad_values], axis=2)
    outgoing = (
        jnp.dot(placed_bf, slot_grad.reshape(slot_count, -1), preferred_element_type=jnp.float32)
        .astype(jnp.bfloat16)
        .reshape(owners, MOST, plen, 2 * kv_width)
    )
    returned = lax.all_to_all(outgoing, "st", split_axis=0, concat_axis=0, tiled=True)
    matched = (jnp.arange(pass_dev, dtype=jnp.int32)[:, None] == wanted[None, :]).astype(
        jnp.bfloat16
    )
    passage_grad = jnp.dot(
        matched, returned.reshape(cells, -1), preferred_element_type=jnp.float32
    ).reshape(pass_dev * plen, 2 * kv_width)
    key_grad = passage_grad[:, :kv_width]
    upper = key_grad.astype(jnp.bfloat16)
    lower = (key_grad - upper.astype(jnp.float32)).astype(jnp.bfloat16)
    key_term = across_rows(store_rows, upper) + across_rows(store_rows, lower)
    grad_key_weight = lax.psum(key_term, "st")
    passage_bf = passage_grad.astype(jnp.bfloat16)
    grad_store = lax.psum_scatter(
        (
            against_rows(passage_bf[:, :kv_width], w_key)
            + against_rows(passage_bf[:, kv_width:], w_value)
        ).astype(jnp.bfloat16),
        "tp",
        scatter_dimension=0,
        tiled=True,
    ).astype(jnp.float32)
    grad_store = grad_store.astype(jnp.bfloat16).reshape(-1, plen, width)
    ret_query = jnp.dot(tokens, w_ret_query, preferred_element_type=jnp.float32).astype(
        jnp.bfloat16
    )
    ret_key = jnp.dot(tokens, w_ret_key, preferred_element_type=jnp.float32).astype(jnp.bfloat16)
    ret_value = jnp.dot(tokens, w_ret_value, preferred_element_type=jnp.float32).astype(
        jnp.bfloat16
    )
    grad_rq, grad_rk, grad_rv = retention_grads(
        ret_query, ret_key, ret_value, ret_rate, ret_gain, out_grad
    )
    total = against_rows(grad_query, w_query)
    total = total + against_rows(grad_rq, w_ret_query)
    total = total + against_rows(grad_rk, w_ret_key)
    grad_tokens = lax.psum_scatter(
        (total + against_rows(grad_rv, w_ret_value)).astype(jnp.bfloat16),
        "tp",
        scatter_dimension=0,
        tiled=True,
    )
    return (grad_tokens, grad_store, grad_key_weight)


PLANE = 4
PARTS = 2
SPAN = 128
CHUNKS = 4
SWAPS = 4
TOGETHER = 4
VMEM_BYTES = 67043328
TILE = 256
BF = jnp.bfloat16
F32 = jnp.float32
MESH = pl.DeviceIdType.MESH


def nn(a, b):
    return lax.dot_general(a, b, (((1,), (0,)), ((), ())), preferred_element_type=F32)


def nt(a, b):
    return lax.dot_general(a, b, (((1,), (1,)), ((), ())), preferred_element_type=F32)


def tn(a, b):
    return lax.dot_general(a, b, (((0,), (0,)), ((), ())), preferred_element_type=F32)


def fused_kernel(
    n,
    ids_hbm,
    rate_hbm,
    gain_hbm,
    gate_hbm,
    tokens_hbm,
    store_hbm,
    wq_hbm,
    wk_hbm,
    wv_hbm,
    wrq_hbm,
    wrk_hbm,
    wrv_hbm,
    og_hbm,
    gt_res,
    gs_res,
    gkw_res,
    ids_ref,
    rate_ref,
    gain_ref,
    gate_ref,
    tokens,
    store,
    wq,
    wk,
    wv,
    wrq,
    wrk,
    wrv,
    og,
    q,
    rq,
    rk,
    rv,
    gq,
    grq,
    grk,
    grv,
    total,
    gt,
    gt_in,
    gs_key,
    gs,
    gs_in,
    ga,
    ga_bf,
    kv_col,
    kv_out,
    kv_in,
    req_out,
    req_in,
    stage_k,
    stage_v,
    gk_out,
    gv_out,
    gk_in,
    v_in,
    vp_out,
    v_mid,
    v_add,
    pk,
    pv,
    slices,
    pk_in,
    p1_sum,
    p2_in,
    kg,
    owner_of,
    slot_of,
    local_of,
    load_sem,
    small_sem,
    tp_send,
    tp_recv,
    req_send,
    req_recv,
    v_send,
    v_recv,
    vp_send,
    vp_recv,
    vm_recv,
    gk_send,
    gk_recv,
    z_send,
    z_recv,
    kv_send,
    kv_recv,
    rows_send,
    rows_recv,
    swap_send,
    swap_recv,
    pk_send,
    pk_recv,
    p2_send,
    p2_recv,
    p3_send,
    p3_recv,
    p4_send,
    p4_recv,
):
    me = lax.axis_index("st")
    tp = lax.axis_index("tp")
    length = tokens.shape[0]
    width = tokens.shape[1]
    plen = kv_in.shape[1]
    pass_dev = store.shape[0] // plen
    blocks = length // BLK
    slots = blocks * KP
    group = q.shape[1] // HEAD
    ret_heads = rate_ref.shape[0]
    depth = n // PLANE
    my_q = lax.rem(me, PLANE)
    my_z = lax.div(me, PLANE)
    half_tok = length // 2
    half_store = store.shape[0] // 2

    pairs = (
        (store_hbm, store),
        (wk_hbm, wk),
        (wv_hbm, wv),
        (tokens_hbm, tokens),
        (wrq_hbm, wrq),
        (wrk_hbm, wrk),
        (wrv_hbm, wrv),
        (og_hbm, og),
        (wq_hbm, wq),
    )
    loads = [pltpu.make_async_copy(a, b, load_sem.at[i]) for i, (a, b) in enumerate(pairs)]
    small = [
        pltpu.make_async_copy(a, b, small_sem.at[i])
        for i, (a, b) in enumerate(
            (
                (ids_hbm, ids_ref),
                (rate_hbm, rate_ref),
                (gain_hbm, gain_ref),
                (gate_hbm, gate_ref),
            )
        )
    ]
    small[0].start()
    for load in loads[:3] + small[1:]:
        load.start()

    barrier = pltpu.get_barrier_semaphore()
    has_up = my_z < depth - 1
    has_down = my_z > 0

    def greet(axis, index):
        pl.semaphore_signal(barrier, inc=1, device_id={axis: index}, device_id_type=MESH)

    @pl.when(has_up)
    def _():
        greet("st", me + PLANE)

    @pl.when(has_down)
    def _():
        greet("st", me - PLANE)

    for i in range(1, PLANE):
        greet("st", my_z * PLANE + lax.rem(my_q + i, PLANE))
    greet("tp", 1 - tp)

    small[0].wait()
    for s in range(slots):
        owner_of[s] = lax.div(ids_ref[s // KP, s % KP], pass_dev)

    def invert(o, carry):
        local = jnp.int32(0)
        where = jnp.int32(0)
        for s in range(slots):
            ident = ids_ref[s // KP, s % KP]
            hit = owner_of[s] == o
            local = jnp.where(hit, lax.rem(ident, pass_dev), local)
            where = jnp.where(hit, jnp.int32(s), where)
        slot_of[o] = where
        local_of[o] = local
        return carry

    lax.fori_loop(0, n, invert, 0)
    row_at = lax.broadcasted_iota(jnp.int32, req_out.shape[1:], 0)
    for c in range(PLANE):
        tile = jnp.zeros(req_out.shape[1:], jnp.int32)
        for z in range(depth):
            tile = jnp.where(row_at == z, local_of[z * PLANE + c], tile)
        req_out[c] = tile

    for load in loads[3:]:
        load.start()

    def peer(i):
        step = lax.div(i, PLANE)
        dz = jnp.where(my_z * 2 < depth, step, lax.rem(depth - step, depth))
        return lax.rem(my_z + dz, depth), lax.rem(my_q + lax.rem(i, PLANE), PLANE)

    def exchange(out_ref, in_ref, send, recv, i):
        z, c = peer(i)
        target = z * PLANE + c
        return pltpu.make_async_remote_copy(
            src_ref=out_ref.at[target],
            dst_ref=in_ref.at[me],
            send_sem=send,
            recv_sem=recv,
            device_id={"st": target},
            device_id_type=MESH,
        )

    def bulk(ref, send, recv):
        return pltpu.make_async_remote_copy(
            src_ref=ref,
            dst_ref=ref,
            send_sem=send,
            recv_sem=recv,
            device_id={"tp": 1 - tp},
            device_id_type=MESH,
        )

    def bulk_all(out_ref, in_ref, send, recv):
        return bulk(in_ref.at[pl.ds(0, n - 1)], send, recv)

    def start_some(lo, hi, *refs):
        def body(i, carry):
            exchange(*refs, i).start()
            return carry

        lax.fori_loop(lo, hi, body, 0)

    def ask(i, far):
        z, c = peer(i)
        return pltpu.make_async_remote_copy(
            src_ref=req_out.at[c],
            dst_ref=req_in.at[me],
            send_sem=req_send.at[far],
            recv_sem=req_recv.at[far],
            device_id={"st": z * PLANE + c},
            device_id_type=MESH,
        )

    asked_near = bulk(req_in.at[pl.ds(0, PLANE - 1)], req_send.at[0], req_recv.at[0])
    asked_far = bulk(req_in.at[pl.ds(0, n - PLANE)], req_send.at[1], req_recv.at[1])
    gks = [
        (gk_out.at[c], gk_in.at[c], gk_send.at[c], gk_recv.at[c]) for c in range(PARTS)
    ]

    pl.semaphore_wait(
        barrier, PLANE + has_up.astype(jnp.int32) + has_down.astype(jnp.int32)
    )
    for i in range(1, PLANE):
        ask(i, 0).start()
    req_in[me] = req_out[my_q]

    grain = plen // CHUNKS

    def grain_of(p):
        return pl.ds(pl.multiple_of(p * grain, grain), grain)

    def along(up, z, p):
        at = kv_col.at[z, :, grain_of(p)]
        return pltpu.make_async_remote_copy(
            src_ref=at,
            dst_ref=at,
            send_sem=z_send.at[up, z],
            recv_sem=z_recv.at[z, p],
            device_id={"st": me + (2 * up - 1) * PLANE},
            device_id_type=MESH,
        )

    for load in loads[:3]:
        load.wait()
    own_shape = (pass_dev, plen, HEAD)
    kv_col[my_z, :, :, :HEAD] = nn(store[...], wk[...]).astype(BF).reshape(own_shape)
    kv_col[my_z, :, :, HEAD:] = nn(store[...], wv[...]).astype(BF).reshape(own_shape)
    for p in range(CHUNKS):

        @pl.when(has_up)
        def _():
            along(1, my_z, p).start()

        @pl.when(has_down)
        def _():
            along(0, my_z, p).start()

    def names(row, p, lanes):
        mask = jnp.where(row == p, 1.0, 0.0).astype(F32)
        return jnp.concatenate([mask] * (lanes // mask.shape[1]), axis=1)

    def hand(z, p, i):
        return pltpu.make_async_remote_copy(
            src_ref=kv_out.at[z, i - 1, grain_of(p)],
            dst_ref=kv_in.at[z * PLANE + my_q, grain_of(p)],
            send_sem=kv_send.at[0],
            recv_sem=kv_recv.at[0],
            device_id={"st": my_z * PLANE + lax.rem(my_q + i, PLANE)},
            device_id_type=MESH,
        )

    def spread(z, p):
        rows = [kv_col[z, k, grain_of(p), :].astype(F32) for k in range(pass_dev)]

        def pick(reader):
            row = req_in[my_z * PLANE + reader, pl.ds(z, 1), :]
            chosen = names(row, 0, 2 * HEAD) * rows[0]
            for k in range(1, pass_dev):
                chosen = chosen + names(row, k, 2 * HEAD) * rows[k]
            return chosen.astype(BF)

        for i in range(1, PLANE):
            kv_out[z, i - 1, grain_of(p), :] = pick(lax.rem(my_q + i, PLANE))
        kv_in[z * PLANE + my_q, grain_of(p), :] = pick(my_q)
        for i in range(1, PLANE):
            hand(z, p, i).start()

    def pump(k, p):
        def side(up, carry):
            z = my_z + k * (1 - 2 * up)

            @pl.when((z >= 0) & (z < depth))
            def _():
                along(up, z, p).wait_recv()

                @pl.when(jnp.where(up == 1, has_up, has_down))
                def _():
                    along(up, z, p).start()

                spread(z, p)

            return carry

        lax.fori_loop(0, 2, side, 0)

    quarter = width // PLANE
    share = quarter // 2

    def share_rows(i):
        other = lax.rem(my_q + i, PLANE)
        return pltpu.make_async_remote_copy(
            src_ref=store.at[:, pl.ds(pl.multiple_of(other * quarter + tp * share, share), share)],
            dst_ref=slices.at[tp, i - 1],
            send_sem=rows_send.at[0],
            recv_sem=rows_recv.at[0],
            device_id={"st": my_z * PLANE + other},
            device_id_type=MESH,
        )

    rows_shared = bulk(slices.at[tp], rows_send.at[0], rows_recv.at[0])
    rows_swap = bulk(slices.at[tp], swap_send.at[0], swap_recv.at[0])
    rows_swapped = bulk(slices.at[1 - tp], swap_send.at[0], swap_recv.at[0])

    def project(w, out, then=None):
        def body(i, carry):
            cols = pl.ds(pl.multiple_of(i * TILE, TILE), TILE)
            out[:, cols] = nn(tokens[...], w[:, cols]).astype(BF)
            if then is not None:
                then(i)
            return carry

        lax.fori_loop(0, w.shape[1] // TILE, body, 0)

    loads[3].wait()
    for load, w, out in ((loads[4], wrq, rq), (loads[5], wrk, rk)):
        load.wait()
        project(w, out)
    asked_near.wait_recv()

    def spread_own(p, carry):
        spread(my_z, p)
        return carry

    lax.fori_loop(0, CHUNKS, spread_own, 0)
    for i in range(1, PLANE):
        share_rows(i).start()
    loads[6].wait()
    project(wrv, rv)
    loads[7].wait()
    for load in small[1:]:
        load.wait()

    ret_key = rq.shape[1] // ret_heads
    ret_value = rv.shape[1] // ret_heads
    at_t = lax.broadcasted_iota(jnp.int32, (length, length), 0)
    at_s = lax.broadcasted_iota(jnp.int32, (length, length), 1)
    distance = (at_t - at_s).astype(F32)

    def retention(j, carry):
        kc = pl.ds(pl.multiple_of(j * ret_key, ret_key), ret_key)
        vc = pl.ds(pl.multiple_of(j * ret_value, ret_value), ret_value)
        damping = jnp.where(
            distance >= 0.0, jnp.exp(-rate_ref[j] * jnp.maximum(distance, 0.0)), 0.0
        ) * ret_key ** (-0.5)
        weights = (nt(rq[:, kc], rk[:, kc]) * damping).astype(BF)
        y = nn(weights, rv[:, vc])
        r = lax.rsqrt(jnp.mean(y * y, axis=1, keepdims=True) + EPSILON)
        c = og[:, vc].astype(F32) * gain_ref[:, vc]
        inner = jnp.mean(c * y, axis=1, keepdims=True)
        gy = (r * c - r * r * r * y * inner).astype(BF)
        gw = (nt(gy, rv[:, vc]) * damping).astype(BF)
        grq[:, kc] = nn(gw, rk[:, kc]).astype(BF)
        grk[:, kc] = tn(gw, rq[:, kc]).astype(BF)
        grv[:, vc] = tn(weights, gy).astype(BF)
        pump(1, j)
        return carry

    lax.fori_loop(0, ret_heads, retention, 0)
    loads[8].wait()
    project(wq, q, lambda i: pump(2, i))

    def ret_total(i, carry):
        wide = width // CHUNKS
        rows = pl.ds(pl.multiple_of(i * wide, wide), wide)
        total[:, rows] = (
            nt(grq[...], wrq[rows, :]) + nt(grk[...], wrk[rows, :]) + nt(grv[...], wrv[rows, :])
        )
        pump(3, i)
        return carry

    lax.fori_loop(0, CHUNKS, ret_total, 0)
    rows_shared.wait_recv()
    rows_swap.start()
    cols = [slice(g * HEAD, (g + 1) * HEAD) for g in range(group)]
    gate = 1.0 / (1.0 + jnp.exp(-gate_ref[...]))

    def gated(b, carry):
        rows = pl.ds(pl.multiple_of(b * BLK, BLK), BLK)
        for g, c in enumerate(cols):
            at = slice(g * BLK, (g + 1) * BLK)
            grad_attn = og[rows, c].astype(F32) * gate[:, c]
            ga[b, at, :] = grad_attn
            ga_bf[b, at, :] = grad_attn.astype(BF)
        return carry

    lax.fori_loop(0, blocks, gated, 0)
    bulk(kv_in.at[pl.ds(0, n - depth)], kv_send.at[0], kv_recv.at[0]).wait_recv()

    def ask_far(i, carry):
        ask(i, 1).start()
        return carry

    lax.fori_loop(PLANE, n, ask_far, 0)
    factor = HEAD ** (-0.5)

    def attend(step, carry):
        group_of = [step * TOGETHER + t for t in range(TOGETHER)]
        rows = [pl.ds(pl.multiple_of(b * BLK, BLK), BLK) for b in group_of]
        read = [[kv_in[owner_of[b * KP + k]] for k in range(KP)] for b in group_of]
        keys = [jnp.concatenate([x[:, :HEAD] for x in each], axis=0) for each in read]
        values = [jnp.concatenate([x[:, HEAD:] for x in each], axis=0) for each in read]
        queries = [jnp.concatenate([q[r, c] for c in cols], axis=0) for r in rows]
        expo = [jnp.exp(nt(a, b) * factor) for a, b in zip(queries, keys)]
        grad_probs = [nt(ga_bf[b], v) for b, v in zip(group_of, values)]
        probs = [e / jnp.sum(e, axis=1, keepdims=True) for e in expo]
        probs_bf = [x.astype(BF) for x in probs]
        attn = [nn(x, v) for x, v in zip(probs_bf, values)]
        delta = [
            jnp.sum(ga[b] * a, axis=1, keepdims=True) for b, a in zip(group_of, attn)
        ]
        scores = [
            (x * (g - d) * factor).astype(BF) for x, g, d in zip(probs, grad_probs, delta)
        ]
        dk = [tn(x, a).astype(BF) for x, a in zip(scores, queries)]
        dv = [tn(x, ga_bf[b]).astype(BF) for x, b in zip(probs_bf, group_of)]
        grad_query = [nn(x, a).astype(BF) for x, a in zip(scores, keys)]
        for t, b in enumerate(group_of):
            for g, c in enumerate(cols):
                gq[rows[t], c] = grad_query[t][g * BLK : (g + 1) * BLK, :]
            for k in range(KP):
                at = slice(k * plen, (k + 1) * plen)
                for c in range(PARTS):
                    stage_k[c, b * KP + k] = dk[t][at, c * SPAN : (c + 1) * SPAN]
                stage_v[b * KP + k] = dv[t][at, :]
        return carry

    lax.fori_loop(0, blocks // TOGETHER, attend, 0)

    def place(stage, out):
        def body(o, carry):
            out[o] = stage[slot_of[o]]
            return carry

        lax.fori_loop(0, n, body, 0)

    is_end = (my_z == 0) | (my_z == depth - 1)
    upper = my_z * 2 >= depth
    near_end = jnp.where(upper, depth - 1, 0)
    near_mid = jnp.where(upper, depth - 2, 1)
    far_end = depth - 1 - near_end
    far_mid = depth - 1 - near_mid

    def hand_value(z, i, part):
        mate = lax.rem(my_q + i, PLANE)
        return pltpu.make_async_remote_copy(
            src_ref=gv_out.at[z * PLANE + mate],
            dst_ref=v_in.at[z, my_q],
            send_sem=v_send.at[part],
            recv_sem=v_recv.at[part],
            device_id={"st": my_z * PLANE + mate},
            device_id_type=MESH,
        )

    place(stage_k.at[0], gk_out.at[0])
    start_some(1, n, *gks[0])
    place(stage_k.at[1], gk_out.at[1])
    place(stage_v, gv_out)
    for c in range(PARTS):
        gk_in[c, me] = gk_out[c, me]
    for z in range(depth):
        v_in[z, my_q] = gv_out[z * PLANE + my_q]

    def finish_total(i, carry):
        rows = pl.ds(pl.multiple_of(i * TILE, TILE), TILE)
        gt[:, rows] = (total[:, rows] + nt(gq[...], wq[rows, :])).astype(BF)
        return carry

    lax.fori_loop(0, width // TILE, finish_total, 0)
    for z in (far_end, far_mid):
        for i in range(1, PLANE):
            hand_value(z, i, 0).start()

    def to_partner(out_ref, in_ref, half, at):
        return pltpu.make_async_remote_copy(
            src_ref=out_ref.at[pl.ds(pl.multiple_of((1 - tp) * half, half), half)],
            dst_ref=in_ref,
            send_sem=tp_send.at[at],
            recv_sem=tp_recv.at[at],
            device_id={"tp": 1 - tp},
            device_id_type=MESH,
        )

    def add_own(out_ref, in_ref, half, res_ref):
        own = out_ref[pl.ds(pl.multiple_of(tp * half, half), half), :]
        res_ref[...] = (own.astype(F32) + in_ref[...].astype(F32)).astype(BF)

    token_swap = to_partner(gt, gt_in, half_tok, 0)
    token_swap.start()

    def gather_sum(in_ref, out_ref):
        lanes = out_ref.shape[1]

        def body(r, sums):
            row = req_in[r, pl.ds(my_z, 1), :]
            term = in_ref[r].astype(F32)
            return tuple(s + names(row, p, lanes) * term for p, s in enumerate(sums))

        sums = lax.fori_loop(0, n, body, (jnp.zeros((plen, lanes), F32),) * pass_dev)
        for p, s in enumerate(sums):
            out_ref[p * plen : (p + 1) * plen, :] = s.astype(BF)

    def share_key(c, i):
        return pltpu.make_async_remote_copy(
            src_ref=pk.at[c],
            dst_ref=pk_in.at[c, i - 1],
            send_sem=pk_send.at[c],
            recv_sem=pk_recv.at[c],
            device_id={"st": my_z * PLANE + lax.rem(my_q + i, PLANE)},
            device_id_type=MESH,
        )

    side = jnp.where(upper, 1, 0)

    def column_reduce(c, which, slot, t):
        return pltpu.make_async_remote_copy(
            src_ref=p1_sum.at[c, which, t],
            dst_ref=p2_in.at[c, t, slot],
            send_sem=p2_send.at[c],
            recv_sem=p2_recv.at[c, t],
            device_id={"st": (1 + which) * PLANE + my_q},
            device_id_type=MESH,
        )

    def column_gather(c, z, which, t):
        at = kg.at[c, my_q * depth + 2 * which + t]
        return pltpu.make_async_remote_copy(
            src_ref=at,
            dst_ref=at,
            send_sem=p3_send.at[c],
            recv_sem=p3_recv.at[c, 2 * which + t],
            device_id={"st": z * PLANE + my_q},
            device_id_type=MESH,
        )

    def plane_gather(c, i, which, t):
        at = kg.at[c, my_q * depth + 2 * which + t]
        return pltpu.make_async_remote_copy(
            src_ref=at,
            dst_ref=at,
            send_sem=p4_send.at[c],
            recv_sem=p4_recv.at[c],
            device_id={"st": my_z * PLANE + lax.rem(my_q + i, PLANE)},
            device_id_type=MESH,
        )

    def rows_of(p):
        return pl.ds(pl.multiple_of(p * plen, plen), plen)

    def send_part(at, dst, sem, z):
        return pltpu.make_async_remote_copy(
            src_ref=at,
            dst_ref=dst,
            send_sem=vp_send.at[0],
            recv_sem=sem,
            device_id={"st": z * PLANE + my_q},
            device_id_type=MESH,
        )

    def merge(z, p, *more):
        acc = jnp.zeros((plen, HEAD), F32)
        for r in range(PLANE):
            row = req_in[my_z * PLANE + r, pl.ds(z, 1), :]
            acc = acc + names(row, p, HEAD) * v_in[z, r].astype(F32)
        for ref in more:
            acc = acc + ref[rows_of(p), :].astype(F32)
        return acc.astype(BF)

    def pass_near():
        z = jnp.where(is_end, near_mid, near_end)

        def body(p, carry):
            vp_out[2, rows_of(p), :] = merge(z, p)
            return carry

        lax.fori_loop(0, pass_dev, body, 0)
        send_part(vp_out.at[2], v_add.at[0], vp_recv.at[0], z).start()

    def pass_first(which):
        z = (far_mid, far_end)[which]

        @pl.when(is_end)
        def _():
            def body(p, carry):
                vp_out[which, rows_of(p), :] = merge(z, p)
                send_part(
                    vp_out.at[which, rows_of(p)],
                    v_mid.at[which, rows_of(p)],
                    vm_recv.at[which, p],
                    near_mid,
                ).start()
                return carry

            lax.fori_loop(0, pass_dev, body, 0)

    def pass_second(which):
        z = (far_mid, far_end)[which]

        @pl.when(jnp.logical_not(is_end))
        def _():
            def body(p, carry):
                at = v_mid.at[which, rows_of(p)]
                bulk(at, vp_send.at[0], vm_recv.at[which, p]).wait_recv()
                vp_out[which, rows_of(p), :] = merge(z, p, v_mid.at[which])
                send_part(
                    vp_out.at[which, rows_of(p)],
                    v_add.at[1, rows_of(p)],
                    vp_recv.at[1],
                    z,
                ).start()
                return carry

            lax.fori_loop(0, pass_dev, body, 0)

    rows_swapped.wait_recv()
    asked_far.wait_recv()

    own_cols = pl.ds(pl.multiple_of(my_q * quarter, quarter), quarter)
    v_half = [bulk(gv_out.at[pl.ds(0, 2 * (PLANE - 1))], v_send.at[h], v_recv.at[h]) for h in range(2)]
    def gather_keys(c):
        bulk_all(*gks[c]).wait_recv()
        if c == 0:
            start_some(1, n, *gks[1])
        gather_sum(gk_in.at[c], pk.at[c])
        for i in range(1, PLANE):
            share_key(c, i).start()

    def key_terms(c):
        own = tn(store[:, own_cols], pk[c])
        bulk(pk_in.at[c], pk_send.at[c], pk_recv.at[c]).wait_recv()
        for part in range(2):
            acc = own[part * share : (part + 1) * share]
            for i in range(1, PLANE):
                acc = acc + tn(slices[part, i - 1], pk_in[c, i - 1])
            p1_sum[c, part] = acc.astype(BF).reshape(p1_sum.shape[2:])

        @pl.when(is_end)
        def _():
            for t in range(2):
                column_reduce(c, 1 - side, 2, t).start()
                column_reduce(c, side, 0, t).start()

        @pl.when(jnp.logical_not(is_end))
        def _():
            for t in range(2):
                column_reduce(c, 1 - side, 1, t).start()

    def reduce_keys(c):
        @pl.when(jnp.logical_not(is_end))
        def _():
            for t in range(2):
                bulk(p2_in.at[c, t], p2_send.at[c], p2_recv.at[c, t]).wait_recv()
                acc = p1_sum[c, side, t].astype(F32)
                for i in range(depth - 1):
                    acc = acc + p2_in[c, t, i].astype(F32)
                kg[c, my_q * depth + 2 * side + t] = acc.astype(BF)
                for z in (far_end, far_mid, near_end):
                    column_gather(c, z, side, t).start()
                for i in range(1, PLANE):
                    plane_gather(c, i, side, t).start()

    def hand_near():
        for z in (near_mid, near_end):
            for i in range(1, PLANE):
                hand_value(z, i, 1).start()

    def finish_tokens():
        token_swap.wait_recv()
        add_own(gt, gt_in, half_tok, gt_res)

    gather_keys(0)
    hand_near()
    v_half[0].wait_recv()
    pass_first(1)
    finish_tokens()
    key_terms(0)
    gather_keys(1)
    reduce_keys(0)
    key_terms(1)
    pass_first(0)
    pass_second(1)
    reduce_keys(1)
    v_half[1].wait_recv()
    pass_near()
    wide = width // SWAPS

    def cut(i):
        return pl.ds(pl.multiple_of(i * wide, wide), wide)

    def fan_out(c, at):
        def body(s, carry):
            keys = jnp.concatenate([pk[e] for e in range(PARTS)], axis=1)
            gs_key[:, cut(at + s)] = nt(keys, wk[cut(at + s), :])
            which = jnp.where(s == 0, side, 1 - side)

            @pl.when(is_end | (s == 1))
            def _():
                for t in range(2):
                    column_gather(c, my_z, which, t).wait_recv()
                    for i in range(1, PLANE):
                        plane_gather(c, i, which, t).start()

            return carry

        lax.fori_loop(0, 2, body, 0)

    fan_out(0, 0)
    pass_second(0)
    fan_out(1, 2)

    for sem in range(2):
        bulk(v_add.at[sem], vp_send.at[0], vp_recv.at[sem]).wait_recv()

    def merge_own(p, carry):
        pv[rows_of(p), :] = merge(my_z, p, v_add.at[0], v_add.at[1])
        return carry

    lax.fori_loop(0, pass_dev, merge_own, 0)

    def half_of(which):
        return pl.ds(pl.multiple_of(which * half_store, half_store), half_store)

    def store_swap(i):
        return pltpu.make_async_remote_copy(
            src_ref=gs.at[half_of(1 - tp), cut(i)],
            dst_ref=gs_in.at[:, cut(i)],
            send_sem=tp_send.at[1 + i],
            recv_sem=tp_recv.at[1 + i],
            device_id={"tp": 1 - tp},
            device_id_type=MESH,
        )

    def store_grad(i, carry):
        gs[:, cut(i)] = (gs_key[:, cut(i)] + nt(pv[...], wv[cut(i), :])).astype(BF)
        store_swap(i).start()
        return carry

    lax.fori_loop(0, SWAPS, store_grad, 0)

    def store_sum(i, carry):
        store_swap(i).wait_recv()
        own = gs[half_of(tp), cut(i)]
        gs_res[:, cut(i)] = (own.astype(F32) + gs_in[:, cut(i)].astype(F32)).astype(BF)
        return carry

    lax.fori_loop(0, SWAPS, store_sum, 0)
    for c in range(PARTS):
        bulk(kg.at[c, pl.ds(0, n - depth)], p4_send.at[c], p4_recv.at[c]).wait_recv()
        gkw_res[:, c * SPAN : (c + 1) * SPAN] = kg[c].reshape(width, SPAN).astype(F32)

    asked_near.wait_send()
    asked_far.wait_send()
    for z in range(depth):

        @pl.when(has_up & (z <= my_z))
        def _():
            bulk(kv_col.at[z], z_send.at[1, z], z_recv.at[z, 0]).wait_send()

        @pl.when(has_down & (z >= my_z))
        def _():
            bulk(kv_col.at[z], z_send.at[0, z], z_recv.at[z, 0]).wait_send()

    bulk(kv_out, kv_send.at[0], kv_recv.at[0]).wait_send()
    for half in v_half:
        half.wait_send()
    bulk(vp_out, vp_send.at[0], vp_recv.at[0]).wait_send()
    token_swap.wait_send()
    for i in range(SWAPS):
        store_swap(i).wait_send()
    for c in range(PARTS):
        bulk_all(*gks[c]).wait_send()
        bulk(pk_in.at[c], pk_send.at[c], pk_recv.at[c]).wait_send()
        bulk(kg.at[c, pl.ds(0, n - depth)], p4_send.at[c], p4_recv.at[c]).wait_send()
    for c in range(PARTS):

        @pl.when(is_end)
        def _():
            bulk(kg.at[c, pl.ds(0, 4)], p2_send.at[c], p4_recv.at[c]).wait_send()

        @pl.when(jnp.logical_not(is_end))
        def _():
            bulk(kg.at[c, pl.ds(0, 2)], p2_send.at[c], p4_recv.at[c]).wait_send()
            bulk(kg.at[c, pl.ds(0, 6)], p3_send.at[c], p4_recv.at[c]).wait_send()

    rows_shared.wait_send()
    rows_swap.wait_send()


def finish_kernel(gt, gs, kg, ot, os, ok, sem):
    copies = [
        pltpu.make_async_copy(a, b, sem.at[i]) for i, (a, b) in enumerate(((kg, ok), (gt, ot), (gs, os)))
    ]
    for copy in copies:
        copy.start()
    for copy in copies:
        copy.wait()


def per_device(sizes, *args):
    (tokens, store, ids, wq, wk, wv, wrq, wrk, wrv, rate, gain, gate, og) = args
    n = sizes["st"]
    pass_dev, plen, width = store.shape
    length = tokens.shape[0]
    rows = pass_dev * plen
    weight_cols = sum(w.shape[1] for w in (wq, wk, wv, wrq, wrk, wrv))
    fits = (
        sizes["tp"] == 2
        and wk.shape[1] == HEAD
        and HEAD == PARTS * SPAN
        and ids.size == n
        and n == PLANE * 4
        and plen % (16 * CHUNKS) == 0
        and length % (BLK * TOGETHER) == 0
        and rate.shape[0] == CHUNKS
        and wq.shape[1] == CHUNKS * TILE
        and width % (n * 128) == 0
        and width * weight_cols + n * plen * HEAD * 12 + length * width * 12 < 24 * 2**20
    )
    if not fits:
        return per_device_plain(*args)
    depth = n // PLANE
    piece = width // n

    def vm(*shape, dtype=BF):
        return pltpu.VMEM(shape, dtype)

    any_spec = pl.BlockSpec(memory_space=pl.ANY)
    vmem = pl.BlockSpec(memory_space=pltpu.VMEM)
    dma = pltpu.SemaphoreType.DMA
    like = [vm(*x.shape) for x in (tokens,)] + [vm(rows, width)]
    like += [vm(*x.shape) for x in (wq, wk, wv, wrq, wrk, wrv, og)]
    qs = [vm(length, w.shape[1]) for w in (wq, wrq, wrk, wrv)]
    scratch = (
        [
            pltpu.SMEM(ids.shape, jnp.int32),
            pltpu.SMEM(rate.shape, F32),
            vm(1, gain.shape[0], dtype=F32),
            vm(1, gate.shape[0], dtype=F32),
        ]
        + like
        + qs
        + qs
        + [
            vm(length, width, dtype=F32),
            vm(length, width),
            vm(length // 2, width),
            vm(rows, width, dtype=F32),
            vm(rows, width),
            vm(rows // 2, width),
            vm(length // BLK, BLK * wq.shape[1] // HEAD, HEAD, dtype=F32),
            vm(length // BLK, BLK * wq.shape[1] // HEAD, HEAD),
            vm(depth, pass_dev, plen, 2 * HEAD),
            vm(depth, PLANE - 1, plen, 2 * HEAD),
            vm(n, plen, 2 * HEAD),
            vm(PLANE, 8, 128, dtype=jnp.int32),
            vm(n, 8, 128, dtype=jnp.int32),
            vm(PARTS, n, plen, SPAN),
            vm(n, plen, HEAD),
            vm(PARTS, n, plen, SPAN),
            vm(n, plen, HEAD),
            vm(PARTS, n, plen, SPAN),
            vm(depth, PLANE, plen, HEAD),
            vm(3, rows, HEAD),
            vm(2, rows, HEAD),
            vm(2, rows, HEAD),
            vm(PARTS, rows, SPAN),
            vm(rows, HEAD),
            vm(2, PLANE - 1, rows, width // (2 * PLANE)),
            vm(PARTS, PLANE - 1, rows, SPAN),
            vm(PARTS, 2, 2, piece, SPAN),
            vm(PARTS, 2, depth - 1, piece, SPAN),
            vm(PARTS, n, piece, SPAN),
            pltpu.SMEM((n,), jnp.int32),
            pltpu.SMEM((n,), jnp.int32),
            pltpu.SMEM((n,), jnp.int32),
            dma((9,)),
            dma((4,)),
        ]
        + [dma((1 + SWAPS,))] * 2
        + [dma((2,))] * 2
        + [dma((2,))] * 2
        + [dma((1,)), dma((2,)), dma((2, pass_dev))]
        + [dma((PARTS,))] * 2
        + [dma((2, depth)), dma((depth, CHUNKS))]
        + [dma((1,))] * 6
        + [dma((PARTS,))] * 3
        + [dma((PARTS, 2)), dma((PARTS,)), dma((PARTS, 4))]
        + [dma((PARTS,))] * 2
    )
    grad_tokens, grad_store, grad_key = pl.pallas_call(
        functools.partial(fused_kernel, n),
        out_shape=(
            pltpu.VMEM((length // 2, width), BF),
            pltpu.VMEM((rows // 2, width), BF),
            pltpu.VMEM((width, HEAD), F32),
        ),
        in_specs=[any_spec] * 13,
        out_specs=(vmem, vmem, vmem),
        scratch_shapes=scratch,
        compiler_params=pltpu.CompilerParams(
            collective_id=0, has_side_effects=True, vmem_limit_bytes=VMEM_BYTES - (length + rows + 4 * HEAD) * width - 2**16
        ),
    )(
        ids,
        rate,
        gain.reshape(1, -1),
        gate.reshape(1, -1),
        tokens,
        store.reshape(rows, width),
        wq,
        wk,
        wv,
        wrq,
        wrk,
        wrv,
        og,
    )
    grad_tokens, grad_store, grad_key = pl.pallas_call(
        finish_kernel,
        out_shape=(
            jax.ShapeDtypeStruct((length // 2, width), BF),
            jax.ShapeDtypeStruct((rows // 2, width), BF),
            jax.ShapeDtypeStruct((width, HEAD), F32),
        ),
        in_specs=[vmem] * 3,
        out_specs=(any_spec, any_spec, any_spec),
        scratch_shapes=[dma((3,))],
        compiler_params=pltpu.CompilerParams(vmem_limit_bytes=8 * 2**20),
    )(grad_tokens, grad_store, grad_key)
    return (grad_tokens, grad_store.reshape(pass_dev // 2, plen, width), grad_key)


def solution(mesh):
    return jax.shard_map(
        functools.partial(per_device, dict(mesh.shape)),
        mesh=mesh,
        in_specs=(
            P("st", None),
            P("st", None, None),
            P("st", None),
            P(None, "tp"),
            P(None, "tp"),
            P(None, "tp"),
            P(None, "tp"),
            P(None, "tp"),
            P(None, "tp"),
            P("tp"),
            P("tp"),
            P("tp"),
            P("st", "tp"),
        ),
        out_specs=(P(("st", "tp"), None), P(("st", "tp"), None, None), P(None, "tp")),
        check_vma=False,
    )
```

```python
import functools

import jax
import jax.numpy as jnp
from jax import lax
from jax.experimental import pallas as pl
from jax.experimental.pallas import tpu as pltpu
from jax.sharding import PartitionSpec as P

HEAD = 256
BLK = 64
KP = 4
MOST = 1


EPSILON = 1.0


def retention_grads(query_rows, key_rows, value_rows, rates, gains, cotangent):
    length = query_rows.shape[0]
    heads = rates.shape[0]
    queries = query_rows.reshape(length, heads, -1)
    keyset = key_rows.reshape(length, heads, -1)
    values = value_rows.reshape(length, heads, -1)
    positions = jnp.arange(length, dtype=jnp.float32)
    distance = positions[:, None] - positions[None, :]
    damping = jnp.where(
        distance >= 0.0, jnp.exp(-rates[:, None, None] * jnp.maximum(distance, 0.0)), 0.0
    ) * queries.shape[-1] ** (-0.5)
    raw = jnp.einsum("thd,shd->hts", queries, keyset, preferred_element_type=jnp.float32)
    weights = (raw * damping).astype(jnp.bfloat16)
    mixed = jnp.einsum("hts,she->the", weights, values, preferred_element_type=jnp.float32)
    inverse = lax.rsqrt(jnp.mean(mixed * mixed, axis=-1, keepdims=True) + EPSILON)
    scaled = cotangent.astype(jnp.float32).reshape(length, heads, -1) * gains.reshape(heads, -1)
    inner = jnp.mean(scaled * mixed, axis=-1, keepdims=True)
    grad_mixed = (inverse * scaled - inverse * inverse * inverse * mixed * inner).astype(
        jnp.bfloat16
    )
    grad_weights = (
        jnp.einsum("the,she->hts", grad_mixed, values, preferred_element_type=jnp.float32) * damping
    ).astype(jnp.bfloat16)
    grad_first = (
        jnp.einsum("hts,shd->thd", grad_weights, keyset, preferred_element_type=jnp.float32)
        .astype(jnp.bfloat16)
        .reshape(length, -1)
    )
    grad_second = (
        jnp.einsum("hts,thd->shd", grad_weights, queries, preferred_element_type=jnp.float32)
        .astype(jnp.bfloat16)
        .reshape(length, -1)
    )
    grad_third = (
        jnp.einsum("hts,the->she", weights, grad_mixed, preferred_element_type=jnp.float32)
        .astype(jnp.bfloat16)
        .reshape(length, -1)
    )
    return (grad_first, grad_second, grad_third)


def against_rows(left, weight):
    return lax.dot_general(
        left, weight, (((1,), (1,)), ((), ())), preferred_element_type=jnp.float32
    )


def across_rows(left, right):
    return lax.dot_general(
        left, right, (((0,), (0,)), ((), ())), preferred_element_type=jnp.float32
    )


def per_device_plain(
    tokens,
    store,
    passage_ids,
    w_query,
    w_key,
    w_value,
    w_ret_query,
    w_ret_key,
    w_ret_value,
    ret_rate,
    ret_gain,
    gate_logit,
    out_grad,
):
    owners = lax.axis_size("st")
    pass_dev, plen, width = store.shape
    length = tokens.shape[0]
    kv_width = w_key.shape[1]
    kv_local = kv_width // HEAD
    group = w_query.shape[1] // HEAD // kv_local
    blocks = length // BLK
    slot_ids = passage_ids.reshape(-1)
    slot_count = slot_ids.shape[0]
    slot_owner = slot_ids // pass_dev
    slot_local = slot_ids % pass_dev
    order = jnp.arange(slot_count, dtype=jnp.int32)
    same_owner = slot_owner[:, None] == slot_owner[None, :]
    rank = jnp.sum(same_owner & (order[None, :] < order[:, None]), axis=1)
    position = slot_owner * MOST + rank
    cells = owners * MOST
    placed = jnp.arange(cells, dtype=jnp.int32)[:, None] == position[None, :]
    request = (jnp.sum(jnp.where(placed, slot_local[None, :] + 1, 0), axis=1) - 1).reshape(
        owners, MOST
    )
    incoming = lax.all_to_all(request, "st", split_axis=0, concat_axis=0, tiled=True)
    wanted = incoming.reshape(-1)
    valid = wanted >= 0
    safe = jnp.maximum(wanted, 0)
    placed_bf = placed.astype(jnp.bfloat16)
    store_rows = store.reshape(-1, width)
    nothing = jnp.zeros((), jnp.bfloat16)
    own_kv = jnp.concatenate(
        [
            jnp.dot(store_rows, w_key, preferred_element_type=jnp.float32).astype(jnp.bfloat16),
            jnp.dot(store_rows, w_value, preferred_element_type=jnp.float32).astype(jnp.bfloat16),
        ],
        axis=1,
    ).reshape(pass_dev, plen, 2 * kv_width)
    reply = jnp.where(valid[:, None, None], own_kv[safe], nothing).reshape(
        owners, MOST, plen, 2 * kv_width
    )
    arrived = lax.all_to_all(reply, "st", split_axis=0, concat_axis=0, tiled=True)
    slot_kv = (
        across_rows(placed_bf, arrived.reshape(cells, -1))
        .astype(jnp.bfloat16)
        .reshape(slot_count, plen, 2 * kv_width)
    )
    factor = HEAD ** (-0.5)
    gate = jax.nn.sigmoid(gate_logit)
    query_bf = jnp.dot(tokens, w_query, preferred_element_type=jnp.float32).astype(jnp.bfloat16)
    queries = query_bf.reshape(blocks, BLK, kv_local, group, HEAD)
    keys = slot_kv[:, :, :kv_width].reshape(blocks, KP * plen, kv_local, HEAD)
    values = slot_kv[:, :, kv_width:].reshape(blocks, KP * plen, kv_local, HEAD)
    scores = (
        jnp.einsum("btkgd,bskd->bkgts", queries, keys, preferred_element_type=jnp.float32) * factor
    )
    expo = jnp.exp(scores)
    probs = expo / jnp.sum(expo, axis=-1, keepdims=True)
    probs_bf = probs.astype(jnp.bfloat16)
    attn = jnp.einsum("bkgts,bskd->btkgd", probs_bf, values, preferred_element_type=jnp.float32)
    grad_attn = out_grad.astype(jnp.float32).reshape(
        blocks, BLK, kv_local, group, HEAD
    ) * gate.reshape(kv_local, group, HEAD)
    grad_attn_bf = grad_attn.astype(jnp.bfloat16)
    grad_probs = jnp.einsum(
        "btkgd,bskd->bkgts", grad_attn_bf, values, preferred_element_type=jnp.float32
    )
    delta = jnp.moveaxis(jnp.sum(grad_attn * attn, axis=-1), 1, 3)
    grad_scores = (probs * (grad_probs - delta[..., None]) * factor).astype(jnp.bfloat16)
    grad_query = (
        jnp.einsum("bkgts,bskd->btkgd", grad_scores, keys, preferred_element_type=jnp.float32)
        .astype(jnp.bfloat16)
        .reshape(length, -1)
    )
    grad_keys = (
        jnp.einsum("bkgts,btkgd->bskd", grad_scores, queries, preferred_element_type=jnp.float32)
        .astype(jnp.bfloat16)
        .reshape(slot_count, plen, kv_width)
    )
    grad_values = (
        jnp.einsum("bkgts,btkgd->bskd", probs_bf, grad_attn_bf, preferred_element_type=jnp.float32)
        .astype(jnp.bfloat16)
        .reshape(slot_count, plen, kv_width)
    )
    slot_grad = jnp.concatenate([grad_keys, grad_values], axis=2)
    outgoing = (
        jnp.dot(placed_bf, slot_grad.reshape(slot_count, -1), preferred_element_type=jnp.float32)
        .astype(jnp.bfloat16)
        .reshape(owners, MOST, plen, 2 * kv_width)
    )
    returned = lax.all_to_all(outgoing, "st", split_axis=0, concat_axis=0, tiled=True)
    matched = (jnp.arange(pass_dev, dtype=jnp.int32)[:, None] == wanted[None, :]).astype(
        jnp.bfloat16
    )
    passage_grad = jnp.dot(
        matched, returned.reshape(cells, -1), preferred_element_type=jnp.float32
    ).reshape(pass_dev * plen, 2 * kv_width)
    key_grad = passage_grad[:, :kv_width]
    upper = key_grad.astype(jnp.bfloat16)
    lower = (key_grad - upper.astype(jnp.float32)).astype(jnp.bfloat16)
    key_term = across_rows(store_rows, upper) + across_rows(store_rows, lower)
    grad_key_weight = lax.psum(key_term, "st")
    passage_bf = passage_grad.astype(jnp.bfloat16)
    grad_store = lax.psum_scatter(
        (
            against_rows(passage_bf[:, :kv_width], w_key)
            + against_rows(passage_bf[:, kv_width:], w_value)
        ).astype(jnp.bfloat16),
        "tp",
        scatter_dimension=0,
        tiled=True,
    ).astype(jnp.float32)
    grad_store = grad_store.astype(jnp.bfloat16).reshape(-1, plen, width)
    ret_query = jnp.dot(tokens, w_ret_query, preferred_element_type=jnp.float32).astype(
        jnp.bfloat16
    )
    ret_key = jnp.dot(tokens, w_ret_key, preferred_element_type=jnp.float32).astype(jnp.bfloat16)
    ret_value = jnp.dot(tokens, w_ret_value, preferred_element_type=jnp.float32).astype(
        jnp.bfloat16
    )
    grad_rq, grad_rk, grad_rv = retention_grads(
        ret_query, ret_key, ret_value, ret_rate, ret_gain, out_grad
    )
    total = against_rows(grad_query, w_query)
    total = total + against_rows(grad_rq, w_ret_query)
    total = total + against_rows(grad_rk, w_ret_key)
    grad_tokens = lax.psum_scatter(
        (total + against_rows(grad_rv, w_ret_value)).astype(jnp.bfloat16),
        "tp",
        scatter_dimension=0,
        tiled=True,
    )
    return (grad_tokens, grad_store, grad_key_weight)


PLANE = 4
PARTS = 2
SPAN = 128
CHUNKS = 4
SWAPS = 2
TOGETHER = 4
VMEM_BYTES = 67043328
TILE = 256
BF = jnp.bfloat16
F32 = jnp.float32
MESH = pl.DeviceIdType.MESH


def nn(a, b):
    return lax.dot_general(a, b, (((1,), (0,)), ((), ())), preferred_element_type=F32)


def nt(a, b):
    return lax.dot_general(a, b, (((1,), (1,)), ((), ())), preferred_element_type=F32)


def tn(a, b):
    return lax.dot_general(a, b, (((0,), (0,)), ((), ())), preferred_element_type=F32)


def fused_kernel(
    n,
    ids_hbm,
    rate_hbm,
    gain_hbm,
    gate_hbm,
    tokens_hbm,
    store_hbm,
    wq_hbm,
    wk_hbm,
    wv_hbm,
    wrq_hbm,
    wrk_hbm,
    wrv_hbm,
    og_hbm,
    gt_res,
    gs_res,
    gkw_res,
    ids_ref,
    rate_ref,
    gain_ref,
    gate_ref,
    tokens,
    store,
    wq,
    wk,
    wv,
    wrq,
    wrk,
    wrv,
    og,
    q,
    rq,
    rk,
    rv,
    gq,
    grq,
    grk,
    grv,
    total,
    gt,
    gt_in,
    gs_key,
    gs,
    gs_in,
    ga,
    ga_bf,
    kv_col,
    kv_out,
    kv_in,
    req_out,
    req_in,
    stage_k,
    stage_v,
    gk_out,
    gv_out,
    gk_in,
    v_in,
    vp_out,
    v_mid,
    v_add,
    pk,
    pv,
    slices,
    pk_in,
    p1_sum,
    p2_in,
    kg,
    owner_of,
    slot_of,
    local_of,
    load_sem,
    small_sem,
    tp_send,
    tp_recv,
    req_send,
    req_recv,
    v_send,
    v_recv,
    vp_send,
    vp_recv,
    vm_recv,
    gk_send,
    gk_recv,
    z_send,
    z_recv,
    kv_send,
    kv_recv,
    rows_send,
    rows_recv,
    swap_send,
    swap_recv,
    pk_send,
    pk_recv,
    p2_send,
    p2_recv,
    p3_send,
    p3_recv,
    p4_send,
    p4_recv,
):
    me = lax.axis_index("st")
    tp = lax.axis_index("tp")
    length = tokens.shape[0]
    width = tokens.shape[1]
    plen = kv_in.shape[1]
    pass_dev = store.shape[0] // plen
    blocks = length // BLK
    slots = blocks * KP
    group = q.shape[1] // HEAD
    ret_heads = rate_ref.shape[0]
    depth = n // PLANE
    my_q = lax.rem(me, PLANE)
    my_z = lax.div(me, PLANE)
    half_tok = length // 2
    half_store = store.shape[0] // 2

    pairs = (
        (store_hbm, store),
        (wk_hbm, wk),
        (wv_hbm, wv),
        (tokens_hbm, tokens),
        (wrq_hbm, wrq),
        (wrk_hbm, wrk),
        (wrv_hbm, wrv),
        (og_hbm, og),
        (wq_hbm, wq),
    )
    loads = [pltpu.make_async_copy(a, b, load_sem.at[i]) for i, (a, b) in enumerate(pairs)]
    small = [
        pltpu.make_async_copy(a, b, small_sem.at[i])
        for i, (a, b) in enumerate(
            (
                (ids_hbm, ids_ref),
                (rate_hbm, rate_ref),
                (gain_hbm, gain_ref),
                (gate_hbm, gate_ref),
            )
        )
    ]
    small[0].start()
    for load in loads[:3] + small[1:]:
        load.start()

    barrier = pltpu.get_barrier_semaphore()
    has_up = my_z < depth - 1
    has_down = my_z > 0

    def greet(axis, index):
        pl.semaphore_signal(barrier, inc=1, device_id={axis: index}, device_id_type=MESH)

    @pl.when(has_up)
    def _():
        greet("st", me + PLANE)

    @pl.when(has_down)
    def _():
        greet("st", me - PLANE)

    for i in range(1, PLANE):
        greet("st", my_z * PLANE + lax.rem(my_q + i, PLANE))
    greet("tp", 1 - tp)

    small[0].wait()
    for s in range(slots):
        owner_of[s] = lax.div(ids_ref[s // KP, s % KP], pass_dev)

    def invert(o, carry):
        local = jnp.int32(0)
        where = jnp.int32(0)
        for s in range(slots):
            ident = ids_ref[s // KP, s % KP]
            hit = owner_of[s] == o
            local = jnp.where(hit, lax.rem(ident, pass_dev), local)
            where = jnp.where(hit, jnp.int32(s), where)
        slot_of[o] = where
        local_of[o] = local
        return carry

    lax.fori_loop(0, n, invert, 0)
    row_at = lax.broadcasted_iota(jnp.int32, req_out.shape[1:], 0)
    for c in range(PLANE):
        tile = jnp.zeros(req_out.shape[1:], jnp.int32)
        for z in range(depth):
            tile = jnp.where(row_at == z, local_of[z * PLANE + c], tile)
        req_out[c] = tile

    for load in loads[3:]:
        load.start()

    def peer(i):
        step = lax.div(i, PLANE)
        dz = jnp.where(my_z * 2 < depth, step, lax.rem(depth - step, depth))
        return lax.rem(my_z + dz, depth), lax.rem(my_q + lax.rem(i, PLANE), PLANE)

    def exchange(out_ref, in_ref, send, recv, i):
        z, c = peer(i)
        target = z * PLANE + c
        return pltpu.make_async_remote_copy(
            src_ref=out_ref.at[target],
            dst_ref=in_ref.at[me],
            send_sem=send,
            recv_sem=recv,
            device_id={"st": target},
            device_id_type=MESH,
        )

    def bulk(ref, send, recv):
        return pltpu.make_async_remote_copy(
            src_ref=ref,
            dst_ref=ref,
            send_sem=send,
            recv_sem=recv,
            device_id={"tp": 1 - tp},
            device_id_type=MESH,
        )

    def bulk_all(out_ref, in_ref, send, recv):
        return bulk(in_ref.at[pl.ds(0, n - 1)], send, recv)

    def start_some(lo, hi, *refs):
        def body(i, carry):
            exchange(*refs, i).start()
            return carry

        lax.fori_loop(lo, hi, body, 0)

    def ask(i, far):
        z, c = peer(i)
        return pltpu.make_async_remote_copy(
            src_ref=req_out.at[c],
            dst_ref=req_in.at[me],
            send_sem=req_send.at[far],
            recv_sem=req_recv.at[far],
            device_id={"st": z * PLANE + c},
            device_id_type=MESH,
        )

    asked_near = bulk(req_in.at[pl.ds(0, PLANE - 1)], req_send.at[0], req_recv.at[0])
    asked_far = bulk(req_in.at[pl.ds(0, n - PLANE)], req_send.at[1], req_recv.at[1])
    gks = [
        (gk_out.at[c], gk_in.at[c], gk_send.at[c], gk_recv.at[c]) for c in range(PARTS)
    ]

    pl.semaphore_wait(
        barrier, PLANE + has_up.astype(jnp.int32) + has_down.astype(jnp.int32)
    )
    for i in range(1, PLANE):
        ask(i, 0).start()
    req_in[me] = req_out[my_q]

    grain = plen // CHUNKS

    def grain_of(p):
        return pl.ds(pl.multiple_of(p * grain, grain), grain)

    def along(up, z, p):
        at = kv_col.at[z, :, grain_of(p)]
        return pltpu.make_async_remote_copy(
            src_ref=at,
            dst_ref=at,
            send_sem=z_send.at[up, z],
            recv_sem=z_recv.at[z, p],
            device_id={"st": me + (2 * up - 1) * PLANE},
            device_id_type=MESH,
        )

    for load in loads[:3]:
        load.wait()
    own_shape = (pass_dev, plen, HEAD)
    kv_col[my_z, :, :, :HEAD] = nn(store[...], wk[...]).astype(BF).reshape(own_shape)
    kv_col[my_z, :, :, HEAD:] = nn(store[...], wv[...]).astype(BF).reshape(own_shape)
    for p in range(CHUNKS):

        @pl.when(has_up)
        def _():
            along(1, my_z, p).start()

        @pl.when(has_down)
        def _():
            along(0, my_z, p).start()

    def names(row, p, lanes):
        mask = jnp.where(row == p, 1.0, 0.0).astype(F32)
        return jnp.concatenate([mask] * (lanes // mask.shape[1]), axis=1)

    def hand(z, p, i):
        return pltpu.make_async_remote_copy(
            src_ref=kv_out.at[z, i - 1, grain_of(p)],
            dst_ref=kv_in.at[z * PLANE + my_q, grain_of(p)],
            send_sem=kv_send.at[0],
            recv_sem=kv_recv.at[0],
            device_id={"st": my_z * PLANE + lax.rem(my_q + i, PLANE)},
            device_id_type=MESH,
        )

    def spread(z, p):
        rows = [kv_col[z, k, grain_of(p), :].astype(F32) for k in range(pass_dev)]

        def pick(reader):
            row = req_in[my_z * PLANE + reader, pl.ds(z, 1), :]
            chosen = names(row, 0, 2 * HEAD) * rows[0]
            for k in range(1, pass_dev):
                chosen = chosen + names(row, k, 2 * HEAD) * rows[k]
            return chosen.astype(BF)

        for i in range(1, PLANE):
            kv_out[z, i - 1, grain_of(p), :] = pick(lax.rem(my_q + i, PLANE))
        kv_in[z * PLANE + my_q, grain_of(p), :] = pick(my_q)
        for i in range(1, PLANE):
            hand(z, p, i).start()

    def pump(k, p):
        def side(up, carry):
            z = my_z + k * (1 - 2 * up)

            @pl.when((z >= 0) & (z < depth))
            def _():
                along(up, z, p).wait_recv()

                @pl.when(jnp.where(up == 1, has_up, has_down))
                def _():
                    along(up, z, p).start()

                spread(z, p)

            return carry

        lax.fori_loop(0, 2, side, 0)

    quarter = width // PLANE
    share = quarter // 2

    def share_rows(i):
        other = lax.rem(my_q + i, PLANE)
        return pltpu.make_async_remote_copy(
            src_ref=store.at[:, pl.ds(pl.multiple_of(other * quarter + tp * share, share), share)],
            dst_ref=slices.at[tp, i - 1],
            send_sem=rows_send.at[0],
            recv_sem=rows_recv.at[0],
            device_id={"st": my_z * PLANE + other},
            device_id_type=MESH,
        )

    rows_shared = bulk(slices.at[tp], rows_send.at[0], rows_recv.at[0])
    rows_swap = bulk(slices.at[tp], swap_send.at[0], swap_recv.at[0])
    rows_swapped = bulk(slices.at[1 - tp], swap_send.at[0], swap_recv.at[0])

    def project(w, out, then=None):
        def body(i, carry):
            cols = pl.ds(pl.multiple_of(i * TILE, TILE), TILE)
            out[:, cols] = nn(tokens[...], w[:, cols]).astype(BF)
            if then is not None:
                then(i)
            return carry

        lax.fori_loop(0, w.shape[1] // TILE, body, 0)

    loads[3].wait()
    for load, w, out in ((loads[4], wrq, rq), (loads[5], wrk, rk)):
        load.wait()
        project(w, out)
    asked_near.wait_recv()

    def spread_own(p, carry):
        spread(my_z, p)
        return carry

    lax.fori_loop(0, CHUNKS, spread_own, 0)
    for i in range(1, PLANE):
        share_rows(i).start()
    loads[6].wait()
    project(wrv, rv)
    loads[7].wait()
    for load in small[1:]:
        load.wait()

    ret_key = rq.shape[1] // ret_heads
    ret_value = rv.shape[1] // ret_heads
    at_t = lax.broadcasted_iota(jnp.int32, (length, length), 0)
    at_s = lax.broadcasted_iota(jnp.int32, (length, length), 1)
    distance = (at_t - at_s).astype(F32)

    def retention(j, carry):
        kc = pl.ds(pl.multiple_of(j * ret_key, ret_key), ret_key)
        vc = pl.ds(pl.multiple_of(j * ret_value, ret_value), ret_value)
        damping = jnp.where(
            distance >= 0.0, jnp.exp(-rate_ref[j] * jnp.maximum(distance, 0.0)), 0.0
        ) * ret_key ** (-0.5)
        weights = (nt(rq[:, kc], rk[:, kc]) * damping).astype(BF)
        y = nn(weights, rv[:, vc])
        r = lax.rsqrt(jnp.mean(y * y, axis=1, keepdims=True) + EPSILON)
        c = og[:, vc].astype(F32) * gain_ref[:, vc]
        inner = jnp.mean(c * y, axis=1, keepdims=True)
        gy = (r * c - r * r * r * y * inner).astype(BF)
        gw = (nt(gy, rv[:, vc]) * damping).astype(BF)
        grq[:, kc] = nn(gw, rk[:, kc]).astype(BF)
        grk[:, kc] = tn(gw, rq[:, kc]).astype(BF)
        grv[:, vc] = tn(weights, gy).astype(BF)
        pump(1, j)
        return carry

    lax.fori_loop(0, ret_heads, retention, 0)
    loads[8].wait()
    project(wq, q, lambda i: pump(2, i))

    def ret_total(i, carry):
        wide = width // CHUNKS
        rows = pl.ds(pl.multiple_of(i * wide, wide), wide)
        total[:, rows] = (
            nt(grq[...], wrq[rows, :]) + nt(grk[...], wrk[rows, :]) + nt(grv[...], wrv[rows, :])
        )
        pump(3, i)
        return carry

    lax.fori_loop(0, CHUNKS, ret_total, 0)
    rows_shared.wait_recv()
    rows_swap.start()
    cols = [slice(g * HEAD, (g + 1) * HEAD) for g in range(group)]
    gate = 1.0 / (1.0 + jnp.exp(-gate_ref[...]))

    def gated(b, carry):
        rows = pl.ds(pl.multiple_of(b * BLK, BLK), BLK)
        for g, c in enumerate(cols):
            at = slice(g * BLK, (g + 1) * BLK)
            grad_attn = og[rows, c].astype(F32) * gate[:, c]
            ga[b, at, :] = grad_attn
            ga_bf[b, at, :] = grad_attn.astype(BF)
        return carry

    lax.fori_loop(0, blocks, gated, 0)
    bulk(kv_in.at[pl.ds(0, n - depth)], kv_send.at[0], kv_recv.at[0]).wait_recv()

    def ask_far(i, carry):
        ask(i, 1).start()
        return carry

    lax.fori_loop(PLANE, n, ask_far, 0)
    factor = HEAD ** (-0.5)

    def attend(step, carry):
        group_of = [step * TOGETHER + t for t in range(TOGETHER)]
        rows = [pl.ds(pl.multiple_of(b * BLK, BLK), BLK) for b in group_of]
        read = [[kv_in[owner_of[b * KP + k]] for k in range(KP)] for b in group_of]
        keys = [jnp.concatenate([x[:, :HEAD] for x in each], axis=0) for each in read]
        values = [jnp.concatenate([x[:, HEAD:] for x in each], axis=0) for each in read]
        queries = [jnp.concatenate([q[r, c] for c in cols], axis=0) for r in rows]
        expo = [jnp.exp(nt(a, b) * factor) for a, b in zip(queries, keys)]
        grad_probs = [nt(ga_bf[b], v) for b, v in zip(group_of, values)]
        probs = [e / jnp.sum(e, axis=1, keepdims=True) for e in expo]
        probs_bf = [x.astype(BF) for x in probs]
        attn = [nn(x, v) for x, v in zip(probs_bf, values)]
        delta = [
            jnp.sum(ga[b] * a, axis=1, keepdims=True) for b, a in zip(group_of, attn)
        ]
        scores = [
            (x * (g - d) * factor).astype(BF) for x, g, d in zip(probs, grad_probs, delta)
        ]
        dk = [tn(x, a).astype(BF) for x, a in zip(scores, queries)]
        dv = [tn(x, ga_bf[b]).astype(BF) for x, b in zip(probs_bf, group_of)]
        grad_query = [nn(x, a).astype(BF) for x, a in zip(scores, keys)]
        for t, b in enumerate(group_of):
            for g, c in enumerate(cols):
                gq[rows[t], c] = grad_query[t][g * BLK : (g + 1) * BLK, :]
            for k in range(KP):
                at = slice(k * plen, (k + 1) * plen)
                for c in range(PARTS):
                    stage_k[c, b * KP + k] = dk[t][at, c * SPAN : (c + 1) * SPAN]
                stage_v[b * KP + k] = dv[t][at, :]
        return carry

    lax.fori_loop(0, blocks // TOGETHER, attend, 0)

    def place(stage, out):
        def body(o, carry):
            out[o] = stage[slot_of[o]]
            return carry

        lax.fori_loop(0, n, body, 0)

    is_end = (my_z == 0) | (my_z == depth - 1)
    upper = my_z * 2 >= depth
    near_end = jnp.where(upper, depth - 1, 0)
    near_mid = jnp.where(upper, depth - 2, 1)
    far_end = depth - 1 - near_end
    far_mid = depth - 1 - near_mid

    def hand_value(z, i, part):
        mate = lax.rem(my_q + i, PLANE)
        return pltpu.make_async_remote_copy(
            src_ref=gv_out.at[z * PLANE + mate],
            dst_ref=v_in.at[z, my_q],
            send_sem=v_send.at[part],
            recv_sem=v_recv.at[part],
            device_id={"st": my_z * PLANE + mate},
            device_id_type=MESH,
        )

    place(stage_k.at[0], gk_out.at[0])
    start_some(1, n, *gks[0])
    place(stage_k.at[1], gk_out.at[1])
    place(stage_v, gv_out)
    for c in range(PARTS):
        gk_in[c, me] = gk_out[c, me]
    for z in range(depth):
        v_in[z, my_q] = gv_out[z * PLANE + my_q]

    for z in (far_end, far_mid):
        for i in range(1, PLANE):
            hand_value(z, i, 0).start()

    def finish_total(i, carry):
        rows = pl.ds(pl.multiple_of(i * TILE, TILE), TILE)
        gt[:, rows] = (total[:, rows] + nt(gq[...], wq[rows, :])).astype(BF)
        return carry

    lax.fori_loop(0, width // TILE, finish_total, 0)

    def to_partner(out_ref, in_ref, half, at):
        return pltpu.make_async_remote_copy(
            src_ref=out_ref.at[pl.ds(pl.multiple_of((1 - tp) * half, half), half)],
            dst_ref=in_ref,
            send_sem=tp_send.at[at],
            recv_sem=tp_recv.at[at],
            device_id={"tp": 1 - tp},
            device_id_type=MESH,
        )

    def add_own(out_ref, in_ref, half, res_ref):
        own = out_ref[pl.ds(pl.multiple_of(tp * half, half), half), :]
        res_ref[...] = (own.astype(F32) + in_ref[...].astype(F32)).astype(BF)

    token_swap = to_partner(gt, gt_in, half_tok, 0)
    token_swap.start()

    def gather_sum(in_ref, out_ref):
        lanes = out_ref.shape[1]

        def body(r, sums):
            row = req_in[r, pl.ds(my_z, 1), :]
            term = in_ref[r].astype(F32)
            return tuple(s + names(row, p, lanes) * term for p, s in enumerate(sums))

        sums = lax.fori_loop(0, n, body, (jnp.zeros((plen, lanes), F32),) * pass_dev)
        for p, s in enumerate(sums):
            out_ref[p * plen : (p + 1) * plen, :] = s.astype(BF)

    def share_key(c, i):
        return pltpu.make_async_remote_copy(
            src_ref=pk.at[c],
            dst_ref=pk_in.at[c, i - 1],
            send_sem=pk_send.at[c],
            recv_sem=pk_recv.at[c],
            device_id={"st": my_z * PLANE + lax.rem(my_q + i, PLANE)},
            device_id_type=MESH,
        )

    side = jnp.where(upper, 1, 0)

    def column_reduce(c, which, slot, t):
        return pltpu.make_async_remote_copy(
            src_ref=p1_sum.at[c, which, t],
            dst_ref=p2_in.at[c, t, slot],
            send_sem=p2_send.at[c],
            recv_sem=p2_recv.at[c, t],
            device_id={"st": (1 + which) * PLANE + my_q},
            device_id_type=MESH,
        )

    def column_gather(c, z, which, t):
        at = kg.at[c, my_q * depth + 2 * which + t]
        return pltpu.make_async_remote_copy(
            src_ref=at,
            dst_ref=at,
            send_sem=p3_send.at[c],
            recv_sem=p3_recv.at[c, 2 * which + t],
            device_id={"st": z * PLANE + my_q},
            device_id_type=MESH,
        )

    def plane_gather(c, i, which, t):
        at = kg.at[c, my_q * depth + 2 * which + t]
        return pltpu.make_async_remote_copy(
            src_ref=at,
            dst_ref=at,
            send_sem=p4_send.at[c],
            recv_sem=p4_recv.at[c],
            device_id={"st": my_z * PLANE + lax.rem(my_q + i, PLANE)},
            device_id_type=MESH,
        )

    def rows_of(p):
        return pl.ds(pl.multiple_of(p * plen, plen), plen)

    def send_part(at, dst, sem, z):
        return pltpu.make_async_remote_copy(
            src_ref=at,
            dst_ref=dst,
            send_sem=vp_send.at[0],
            recv_sem=sem,
            device_id={"st": z * PLANE + my_q},
            device_id_type=MESH,
        )

    def merge(z, p, *more):
        acc = jnp.zeros((plen, HEAD), F32)
        for r in range(PLANE):
            row = req_in[my_z * PLANE + r, pl.ds(z, 1), :]
            acc = acc + names(row, p, HEAD) * v_in[z, r].astype(F32)
        for ref in more:
            acc = acc + ref[rows_of(p), :].astype(F32)
        return acc.astype(BF)

    def pass_near():
        z = jnp.where(is_end, near_mid, near_end)

        def body(p, carry):
            vp_out[2, rows_of(p), :] = merge(z, p)
            return carry

        lax.fori_loop(0, pass_dev, body, 0)
        send_part(vp_out.at[2], v_add.at[0], vp_recv.at[0], z).start()

    def pass_first(which):
        z = (far_mid, far_end)[which]

        @pl.when(is_end)
        def _():
            def body(p, carry):
                vp_out[which, rows_of(p), :] = merge(z, p)
                send_part(
                    vp_out.at[which, rows_of(p)],
                    v_mid.at[which, rows_of(p)],
                    vm_recv.at[which, p],
                    near_mid,
                ).start()
                return carry

            lax.fori_loop(0, pass_dev, body, 0)

    def pass_second(which):
        z = (far_mid, far_end)[which]

        @pl.when(jnp.logical_not(is_end))
        def _():
            def body(p, carry):
                at = v_mid.at[which, rows_of(p)]
                bulk(at, vp_send.at[0], vm_recv.at[which, p]).wait_recv()
                vp_out[which, rows_of(p), :] = merge(z, p, v_mid.at[which])
                send_part(
                    vp_out.at[which, rows_of(p)],
                    v_add.at[1, rows_of(p)],
                    vp_recv.at[1],
                    z,
                ).start()
                return carry

            lax.fori_loop(0, pass_dev, body, 0)

    rows_swapped.wait_recv()
    asked_far.wait_recv()

    own_cols = pl.ds(pl.multiple_of(my_q * quarter, quarter), quarter)
    v_half = [bulk(gv_out.at[pl.ds(0, 2 * (PLANE - 1))], v_send.at[h], v_recv.at[h]) for h in range(2)]
    def gather_keys(c):
        bulk_all(*gks[c]).wait_recv()
        if c == 0:
            start_some(1, n, *gks[1])
        gather_sum(gk_in.at[c], pk.at[c])
        for i in range(1, PLANE):
            share_key(c, i).start()

    def key_terms(c):
        own = tn(store[:, own_cols], pk[c])
        bulk(pk_in.at[c], pk_send.at[c], pk_recv.at[c]).wait_recv()
        for part in range(2):
            acc = own[part * share : (part + 1) * share]
            for i in range(1, PLANE):
                acc = acc + tn(slices[part, i - 1], pk_in[c, i - 1])
            p1_sum[c, part] = acc.astype(BF).reshape(p1_sum.shape[2:])

        @pl.when(is_end)
        def _():
            for t in range(2):
                column_reduce(c, 1 - side, 2, t).start()
                column_reduce(c, side, 0, t).start()

        @pl.when(jnp.logical_not(is_end))
        def _():
            for t in range(2):
                column_reduce(c, 1 - side, 1, t).start()

    def reduce_keys(c):
        @pl.when(jnp.logical_not(is_end))
        def _():
            for t in range(2):
                bulk(p2_in.at[c, t], p2_send.at[c], p2_recv.at[c, t]).wait_recv()
                acc = p1_sum[c, side, t].astype(F32)
                for i in range(depth - 1):
                    acc = acc + p2_in[c, t, i].astype(F32)
                kg[c, my_q * depth + 2 * side + t] = acc.astype(BF)
                for z in (far_end, far_mid, near_end):
                    column_gather(c, z, side, t).start()
                for i in range(1, PLANE):
                    plane_gather(c, i, side, t).start()

    def hand_near():
        for z in (near_mid, near_end):
            for i in range(1, PLANE):
                hand_value(z, i, 1).start()

    def finish_tokens():
        token_swap.wait_recv()
        add_own(gt, gt_in, half_tok, gt_res)

    gather_keys(0)
    hand_near()
    v_half[0].wait_recv()
    pass_first(1)
    finish_tokens()
    key_terms(0)
    gather_keys(1)
    reduce_keys(0)
    key_terms(1)
    pass_first(0)
    pass_second(1)
    wide = width // SWAPS

    def cut(i):
        return pl.ds(pl.multiple_of(i * wide, wide), wide)

    def key_store_grad(i, carry):
        keys = jnp.concatenate([pk[e] for e in range(PARTS)], axis=1)
        gs_key[:, cut(i)] = nt(keys, wk[cut(i), :])
        return carry

    lax.fori_loop(0, SWAPS, key_store_grad, 0)
    reduce_keys(1)
    v_half[1].wait_recv()
    pass_near()
    def fan_out(c):
        def body(s, carry):
            which = jnp.where(s == 0, side, 1 - side)

            @pl.when(is_end | (s == 1))
            def _():
                for t in range(2):
                    column_gather(c, my_z, which, t).wait_recv()
                    for i in range(1, PLANE):
                        plane_gather(c, i, which, t).start()

            return carry

        lax.fori_loop(0, 2, body, 0)

    fan_out(0)
    pass_second(0)
    fan_out(1)

    for sem in range(2):
        bulk(v_add.at[sem], vp_send.at[0], vp_recv.at[sem]).wait_recv()

    def merge_own(p, carry):
        pv[rows_of(p), :] = merge(my_z, p, v_add.at[0], v_add.at[1])
        return carry

    lax.fori_loop(0, pass_dev, merge_own, 0)

    def half_of(which):
        return pl.ds(pl.multiple_of(which * half_store, half_store), half_store)

    def store_swap(i):
        return pltpu.make_async_remote_copy(
            src_ref=gs.at[half_of(1 - tp), cut(i)],
            dst_ref=gs_in.at[:, cut(i)],
            send_sem=tp_send.at[1 + i],
            recv_sem=tp_recv.at[1 + i],
            device_id={"tp": 1 - tp},
            device_id_type=MESH,
        )

    def store_grad(i, carry):
        gs[:, cut(i)] = (gs_key[:, cut(i)] + nt(pv[...], wv[cut(i), :])).astype(BF)
        store_swap(i).start()
        return carry

    lax.fori_loop(0, SWAPS, store_grad, 0)

    def store_sum(i, carry):
        store_swap(i).wait_recv()
        own = gs[half_of(tp), cut(i)]
        gs_res[:, cut(i)] = (own.astype(F32) + gs_in[:, cut(i)].astype(F32)).astype(BF)
        return carry

    lax.fori_loop(0, SWAPS, store_sum, 0)
    for c in range(PARTS):
        bulk(kg.at[c, pl.ds(0, n - depth)], p4_send.at[c], p4_recv.at[c]).wait_recv()
        gkw_res[:, c * SPAN : (c + 1) * SPAN] = kg[c].reshape(width, SPAN).astype(F32)

    asked_near.wait_send()
    asked_far.wait_send()
    for z in range(depth):

        @pl.when(has_up & (z <= my_z))
        def _():
            bulk(kv_col.at[z], z_send.at[1, z], z_recv.at[z, 0]).wait_send()

        @pl.when(has_down & (z >= my_z))
        def _():
            bulk(kv_col.at[z], z_send.at[0, z], z_recv.at[z, 0]).wait_send()

    bulk(kv_out, kv_send.at[0], kv_recv.at[0]).wait_send()
    for half in v_half:
        half.wait_send()
    bulk(vp_out, vp_send.at[0], vp_recv.at[0]).wait_send()
    token_swap.wait_send()
    for i in range(SWAPS):
        store_swap(i).wait_send()
    for c in range(PARTS):
        bulk_all(*gks[c]).wait_send()
        bulk(pk_in.at[c], pk_send.at[c], pk_recv.at[c]).wait_send()
        bulk(kg.at[c, pl.ds(0, n - depth)], p4_send.at[c], p4_recv.at[c]).wait_send()
    for c in range(PARTS):

        @pl.when(is_end)
        def _():
            bulk(kg.at[c, pl.ds(0, 4)], p2_send.at[c], p4_recv.at[c]).wait_send()

        @pl.when(jnp.logical_not(is_end))
        def _():
            bulk(kg.at[c, pl.ds(0, 2)], p2_send.at[c], p4_recv.at[c]).wait_send()
            bulk(kg.at[c, pl.ds(0, 6)], p3_send.at[c], p4_recv.at[c]).wait_send()

    rows_shared.wait_send()
    rows_swap.wait_send()


def finish_kernel(gt, gs, kg, ot, os, ok, sem):
    span = kg.shape[0] // 4
    pairs = [(kg.at[pl.ds(i * span, span)], ok.at[pl.ds(i * span, span)]) for i in range(4)]
    pairs += [(gt, ot), (gs, os)]
    copies = [pltpu.make_async_copy(a, b, sem.at[i]) for i, (a, b) in enumerate(pairs)]
    for copy in copies:
        copy.start()
    for copy in copies:
        copy.wait()


def per_device(sizes, *args):
    (tokens, store, ids, wq, wk, wv, wrq, wrk, wrv, rate, gain, gate, og) = args
    n = sizes["st"]
    pass_dev, plen, width = store.shape
    length = tokens.shape[0]
    rows = pass_dev * plen
    weight_cols = sum(w.shape[1] for w in (wq, wk, wv, wrq, wrk, wrv))
    fits = (
        sizes["tp"] == 2
        and wk.shape[1] == HEAD
        and HEAD == PARTS * SPAN
        and ids.size == n
        and n == PLANE * 4
        and plen % (16 * CHUNKS) == 0
        and length % (BLK * TOGETHER) == 0
        and rate.shape[0] == CHUNKS
        and wq.shape[1] == CHUNKS * TILE
        and width % (n * 128) == 0
        and width * weight_cols + n * plen * HEAD * 12 + length * width * 12 < 24 * 2**20
    )
    if not fits:
        return per_device_plain(*args)
    depth = n // PLANE
    piece = width // n

    def vm(*shape, dtype=BF):
        return pltpu.VMEM(shape, dtype)

    any_spec = pl.BlockSpec(memory_space=pl.ANY)
    vmem = pl.BlockSpec(memory_space=pltpu.VMEM)
    dma = pltpu.SemaphoreType.DMA
    like = [vm(*x.shape) for x in (tokens,)] + [vm(rows, width)]
    like += [vm(*x.shape) for x in (wq, wk, wv, wrq, wrk, wrv, og)]
    qs = [vm(length, w.shape[1]) for w in (wq, wrq, wrk, wrv)]
    scratch = (
        [
            pltpu.SMEM(ids.shape, jnp.int32),
            pltpu.SMEM(rate.shape, F32),
            vm(1, gain.shape[0], dtype=F32),
            vm(1, gate.shape[0], dtype=F32),
        ]
        + like
        + qs
        + qs
        + [
            vm(length, width, dtype=F32),
            vm(length, width),
            vm(length // 2, width),
            vm(rows, width, dtype=F32),
            vm(rows, width),
            vm(rows // 2, width),
            vm(length // BLK, BLK * wq.shape[1] // HEAD, HEAD, dtype=F32),
            vm(length // BLK, BLK * wq.shape[1] // HEAD, HEAD),
            vm(depth, pass_dev, plen, 2 * HEAD),
            vm(depth, PLANE - 1, plen, 2 * HEAD),
            vm(n, plen, 2 * HEAD),
            vm(PLANE, 8, 128, dtype=jnp.int32),
            vm(n, 8, 128, dtype=jnp.int32),
            vm(PARTS, n, plen, SPAN),
            vm(n, plen, HEAD),
            vm(PARTS, n, plen, SPAN),
            vm(n, plen, HEAD),
            vm(PARTS, n, plen, SPAN),
            vm(depth, PLANE, plen, HEAD),
            vm(3, rows, HEAD),
            vm(2, rows, HEAD),
            vm(2, rows, HEAD),
            vm(PARTS, rows, SPAN),
            vm(rows, HEAD),
            vm(2, PLANE - 1, rows, width // (2 * PLANE)),
            vm(PARTS, PLANE - 1, rows, SPAN),
            vm(PARTS, 2, 2, piece, SPAN),
            vm(PARTS, 2, depth - 1, piece, SPAN),
            vm(PARTS, n, piece, SPAN),
            pltpu.SMEM((n,), jnp.int32),
            pltpu.SMEM((n,), jnp.int32),
            pltpu.SMEM((n,), jnp.int32),
            dma((9,)),
            dma((4,)),
        ]
        + [dma((1 + SWAPS,))] * 2
        + [dma((2,))] * 2
        + [dma((2,))] * 2
        + [dma((1,)), dma((2,)), dma((2, pass_dev))]
        + [dma((PARTS,))] * 2
        + [dma((2, depth)), dma((depth, CHUNKS))]
        + [dma((1,))] * 6
        + [dma((PARTS,))] * 3
        + [dma((PARTS, 2)), dma((PARTS,)), dma((PARTS, 4))]
        + [dma((PARTS,))] * 2
    )
    grad_tokens, grad_store, grad_key = pl.pallas_call(
        functools.partial(fused_kernel, n),
        out_shape=(
            pltpu.VMEM((length // 2, width), BF),
            pltpu.VMEM((rows // 2, width), BF),
            pltpu.VMEM((width, HEAD), F32),
        ),
        in_specs=[any_spec] * 13,
        out_specs=(vmem, vmem, vmem),
        scratch_shapes=scratch,
        compiler_params=pltpu.CompilerParams(
            collective_id=0, has_side_effects=True, vmem_limit_bytes=VMEM_BYTES - (length + rows + 4 * HEAD) * width - 2**16
        ),
    )(
        ids,
        rate,
        gain.reshape(1, -1),
        gate.reshape(1, -1),
        tokens,
        store.reshape(rows, width),
        wq,
        wk,
        wv,
        wrq,
        wrk,
        wrv,
        og,
    )
    grad_tokens, grad_store, grad_key = pl.pallas_call(
        finish_kernel,
        out_shape=(
            jax.ShapeDtypeStruct((length // 2, width), BF),
            jax.ShapeDtypeStruct((rows // 2, width), BF),
            jax.ShapeDtypeStruct((width, HEAD), F32),
        ),
        in_specs=[vmem] * 3,
        out_specs=(any_spec, any_spec, any_spec),
        scratch_shapes=[dma((6,))],
        compiler_params=pltpu.CompilerParams(vmem_limit_bytes=8 * 2**20),
    )(grad_tokens, grad_store, grad_key)
    return (grad_tokens, grad_store.reshape(pass_dev // 2, plen, width), grad_key)


def solution(mesh):
    return jax.shard_map(
        functools.partial(per_device, dict(mesh.shape)),
        mesh=mesh,
        in_specs=(
            P("st", None),
            P("st", None, None),
            P("st", None),
            P(None, "tp"),
            P(None, "tp"),
            P(None, "tp"),
            P(None, "tp"),
            P(None, "tp"),
            P(None, "tp"),
            P("tp"),
            P("tp"),
            P("tp"),
            P("st", "tp"),
        ),
        out_specs=(P(("st", "tp"), None), P(("st", "tp"), None, None), P(None, "tp")),
        check_vma=False,
    )
```
